32 devices in a mesh: ep: 4 (over y, x), tp: 8 (over z, core).
Axes of the slice: x: 2, y: 2, z: 4, core: 2. Of those that a mesh axis runs over, the one named last changes fastest.
Arguments:
- tokens: bfloat16 [1024, 2048], P('ep'), may hold values from -6 to 6
- cotangent: bfloat16 [1024, 2048], P('ep'), may hold values from -6 to 6
- group_prob: float32 [1024], P('ep'), may hold values from 0.25 to 1
- expert_prob: float32 [1024, 2], P('ep'), may hold values from 0.1 to 1
- routing: int32 [1024, 2], P('ep'), may hold values from 0 to 3, all different within a row; in each aligned block of 256 rows (0 to 255, 256 to 511, ...) at most 192 rows name the same one
- gate_weight: bfloat16 [4, 2048, 4096], P('ep', None, 'tp'), may hold values from -0.125 to 0.125
- up_weight: bfloat16 [4, 2048, 4096], P('ep', None, 'tp'), may hold values from -0.125 to 0.125
- down_weight: bfloat16 [4, 4096, 2048], P('ep', 'tp'), may hold values from -1 to 1
Outputs:
- token_grad: bfloat16 [1024, 2048], P('ep')
- group_prob_grad: float32 [1024], P('ep')
- expert_prob_grad: float32 [1024, 2], P('ep')
- gate_weight_grad: bfloat16 [4, 2048, 4096], P('ep', None, 'tp')
- up_weight_grad: bfloat16 [4, 2048, 4096], P('ep', None, 'tp')
- down_weight_grad: bfloat16 [4, 4096, 2048], P('ep', 'tp')
- gate_row_norms: float32 [4, 2048], P('ep')
- up_row_norms: float32 [4, 2048], P('ep')
- down_row_norms: float32 [4, 4096], P('ep', 'tp')
The draws below stay inside these ranges and needn't reach their ends.
Inputs may be any that keep to these rules, and one draw needn't show every extreme that they name: `routing`: each row names 2 different experts. In each aligned block of 256 rows no expert is named by more than 192 rows, and in every draw some expert is named by exactly 192 rows of some block.
All inputs are finite; a program needn't handle non-finite values.
Results may differ from the reference program's by a relative error of at most 0.0065.
Values may be sent and summed in bfloat16 or wider, within the bound.
A program may use at most 64 MiB of HBM per device.

```python
import math
import jax
import jax.numpy as jnp
import numpy as np
from jax import lax

D = 2048
FF = 4096
TOP_K = 2
TOK_DEV = 256
EXPERTS = 4
CAP = 192
TOKENS = 1024
N_EP = 4


def draw_down_weight(key, part):
    first, second = jax.random.split(key, 2)
    base = jax.random.normal(first, (EXPERTS, FF, D), jnp.float32)
    rough = jax.random.uniform(second, (EXPERTS, FF, 1), jnp.float32, 0.0, 1.0)
    position = jnp.arange(FF, dtype=jnp.float32).reshape(1, FF, 1) / FF
    log_scale = jnp.log(10.0) * (rough - 0.5) + jnp.log(3.0) * (position - 0.5)
    scale = jnp.exp(log_scale)
    scale = scale / jnp.sqrt(jnp.mean(scale * scale, axis=1, keepdims=True))
    values = jnp.clip(base * scale * FF ** (-0.5), -1.0, 1.0)
    return values.astype(jnp.bfloat16)


def block_scale(rng, dims, cuts, smallest, largest):
    factor_of = 1.0
    for axis_at, parts in cuts:
        steps = jax.random.uniform(jax.random.fold_in(jax.random.fold_in(rng, 6), axis_at), (parts,), jnp.float32, smallest / len(cuts), largest / len(cuts))
        factor_of = factor_of * jnp.repeat(jnp.exp(steps), dims[axis_at] // parts).reshape((-1,) + (1,) * (len(dims) - 1 - axis_at))
    return factor_of


def assign_block(rng, own, number, rows, amount, top, bound, skew):
    ranking = jax.random.permutation(rng, amount)
    heavy_load, ordinary = portions_of(amount, rows * top, bound, skew, True), portions_of(amount, rows * top, bound, skew, False)
    places = jnp.arange(amount)

    def named(lengths, offset_by):
        used = int((lengths > 0).sum())
        fixed = max(1, used // 4)
        passed = fixed + (places - fixed + offset_by * (used - fixed)) % max(1, amount - fixed)
        return jnp.zeros((amount,), jnp.int32).at[ranking[jnp.where(places < fixed, places, passed)]].set(jnp.asarray(lengths, jnp.int32))

    lengths = jnp.where(number % 4 == 0, named(heavy_load, number // 4), named(ordinary, number - number // 4 - 1))
    mixed = jax.random.permutation(jax.random.fold_in(own, 3), amount)
    donor, sink = mixed[0:amount // 2 * 2:2], mixed[1:amount // 2 * 2:2]
    margin = jnp.minimum(lengths[donor] - 1, bound - lengths[sink]) // 2
    margin = jnp.where((donor == ranking[0]) | (sink == ranking[0]) | (lengths[sink] == 0), 0, jnp.maximum(margin, 0))
    passed = jax.random.randint(jax.random.fold_in(own, 4), (amount // 2,), 0, 1 << 20) % (margin + 1)
    lengths = lengths.at[donor].add(-passed).at[sink].add(passed)
    labels = jnp.searchsorted(jnp.cumsum(lengths), jnp.arange(rows * top), side="right").astype(jnp.int32)
    grid = labels.reshape(top, rows).T
    grid = grid[jax.random.permutation(jax.random.fold_in(own, 1), rows)]
    offset_by = jax.random.randint(jax.random.fold_in(own, 2), (rows, 1), 0, top)
    return jnp.take_along_axis(grid, (jnp.arange(top)[None, :] + offset_by) % top, axis=1)


def portions_of(count, total, reach, skew, full):
    portions = [(1 << 20) // math.isqrt(grade ** skew) + 1 for grade in range(1, count + 1)]
    largest = reach if full else min(reach, max(-(-total // count), total * portions[0] // sum(portions)))
    least = 1 if total - largest >= count - 1 else 0
    holding, surplus = [largest] + [least] * (count - 1), total - largest - least * (count - 1)
    while surplus > 0:
        movable = [i for i in range(1, count) if holding[i] < largest] or [i for i in range(1, count) if holding[i] < reach]
        pool, left = sum([portions[i] for i in movable]), surplus
        for i in movable:
            more = min(reach - holding[i], max(1, left * portions[i] // pool), surplus)
            holding[i] = holding[i] + more
            surplus = surplus - more
    return np.array(holding)


def bell_draw(own_key, dims, deviation, bound, shards=(), kind=jnp.bfloat16):
    gain = block_scale(own_key, dims, shards, -0.22, 0.18) if shards else 1.0
    array = jax.random.normal(own_key, dims, jnp.float32) * deviation * gain
    return jnp.minimum(jnp.maximum(array, -bound), bound).astype(kind)


def setup_inputs(seed: int = 0) -> dict:
    key_of = jax.random.split(jax.random.key(seed), 9)
    tokens = bell_draw(key_of[0], (TOKENS, D), 1.0, 6.0, ((0, 4),))
    cotangent = bell_draw(key_of[1], (TOKENS, D), 1.0, 6.0, ((0, 4),))
    group_prob = jnp.clip(0.25 + 0.75 * jax.random.uniform(key_of[2], (TOKENS,), jnp.float32) ** block_scale(key_of[2], (TOKENS,), ((0, 4),), -0.2, 0.2), 0.25, 1.0)
    expert_prob = jnp.clip(0.1 + 0.9 * jax.random.uniform(key_of[3], (TOKENS, TOP_K), jnp.float32) ** block_scale(key_of[3], (TOKENS, TOP_K), ((0, 4),), -0.2, 0.2), 0.1, 1.0)
    routing_keys = jax.random.split(jax.random.fold_in(key_of[4], 1), TOKENS // TOK_DEV)
    routing_turns = jax.random.permutation(jax.random.fold_in(key_of[4], 3), TOKENS // TOK_DEV)
    routing = jax.vmap(lambda own, number: assign_block(jax.random.fold_in(key_of[4], 2), own, number, TOK_DEV, EXPERTS, TOP_K, CAP, 2))(routing_keys, routing_turns).reshape((TOKENS, TOP_K))
    gate_weight = bell_draw(key_of[5], (EXPERTS, D, FF), D ** -0.5, 0.125, ((0, 4), (2, 8)))
    up_weight = bell_draw(key_of[6], (EXPERTS, D, FF), D ** -0.5, 0.125, ((0, 4), (2, 8)))
    down_weight = draw_down_weight(jax.random.fold_in(key_of[8], 71), 0)
    return {"tokens": tokens, "cotangent": cotangent, "group_prob": group_prob, "expert_prob": expert_prob, "routing": routing, "gate_weight": gate_weight, "up_weight": up_weight, "down_weight": down_weight}


def slot_targets(route_block):
    flat = route_block.reshape(-1).astype(jnp.int32)
    names = jnp.arange(EXPERTS, dtype=jnp.int32)
    onehot = (flat[:, None] == names[None, :]).astype(jnp.int32)
    before = (jnp.cumsum(onehot, axis=0) - onehot).astype(jnp.int32)
    place = jnp.sum(before * onehot, axis=1).astype(jnp.int32)
    return (flat * CAP + place).astype(jnp.int32)


def expert_pass(operands):
    rows_in, rows_scaled, w_gate, w_up, w_down = operands
    pre_gate = jnp.dot(rows_in, w_gate, preferred_element_type=jnp.float32)
    pre_up = jnp.dot(rows_in, w_up, preferred_element_type=jnp.float32)
    sigma = jax.nn.sigmoid(pre_gate)
    activated = pre_gate * sigma
    derivative = sigma * (1.0 + pre_gate * (1.0 - sigma))
    hidden = (activated * pre_up).astype(jnp.bfloat16)
    hidden_grad = jnp.dot(rows_scaled, w_down.T, preferred_element_type=jnp.float32)
    score = jnp.sum(hidden.astype(jnp.float32) * hidden_grad, axis=1)
    gate_pre = (hidden_grad * pre_up * derivative).astype(jnp.bfloat16)
    up_pre = (hidden_grad * activated).astype(jnp.bfloat16)
    down_sum = jnp.dot(hidden.T, rows_scaled, preferred_element_type=jnp.float32)
    gate_sum = jnp.dot(rows_in.T, gate_pre, preferred_element_type=jnp.float32)
    up_sum = jnp.dot(rows_in.T, up_pre, preferred_element_type=jnp.float32)
    slot_grad = jnp.dot(gate_pre, w_gate.T, preferred_element_type=jnp.float32)
    slot_grad = (slot_grad + jnp.dot(up_pre, w_up.T, preferred_element_type=jnp.float32)).astype(jnp.bfloat16)
    gate_norm = jnp.sum(gate_sum * gate_sum, axis=1) / FF
    up_norm = jnp.sum(up_sum * up_sum, axis=1) / FF
    down_norm = jnp.sum(down_sum * down_sum, axis=1) / D
    return (slot_grad, score, gate_sum.astype(jnp.bfloat16), up_sum.astype(jnp.bfloat16),
            down_sum.astype(jnp.bfloat16), gate_norm, up_norm, down_norm)


def to_experts(buffer):
    tail = buffer.shape[2:]
    shaped = buffer.reshape((N_EP, EXPERTS, CAP) + tail)
    shaped = jnp.swapaxes(shaped, 0, 1)
    return shaped.reshape((EXPERTS, N_EP * CAP) + tail)


def to_blocks(buffer):
    tail = buffer.shape[2:]
    shaped = buffer.reshape((EXPERTS, N_EP, CAP) + tail)
    shaped = jnp.swapaxes(shaped, 0, 1)
    return shaped.reshape((N_EP, EXPERTS * CAP) + tail)


def reference(tokens, cotangent, group_prob, expert_prob, routing, gate_weight, up_weight, down_weight):
    slot_count = TOK_DEV * TOP_K
    blocks = routing.reshape(N_EP, TOK_DEV, TOP_K)
    target = jax.vmap(slot_targets)(blocks)
    source = jnp.broadcast_to(jnp.arange(N_EP, dtype=jnp.int32)[:, None], target.shape)
    weight = group_prob[:, None] * expert_prob
    scaled = (weight[:, :, None] * cotangent.astype(jnp.float32)[:, None, :]).astype(jnp.bfloat16)
    token_slots = jnp.broadcast_to(tokens.reshape(N_EP, TOK_DEV, 1, D), (N_EP, TOK_DEV, TOP_K, D))
    token_slots = token_slots.reshape(N_EP, slot_count, D)
    scaled_slots = scaled.reshape(N_EP, slot_count, D)
    rows_in = jnp.zeros((N_EP, EXPERTS * CAP, D), jnp.bfloat16).at[source, target].set(token_slots)
    rows_scaled = jnp.zeros((N_EP, EXPERTS * CAP, D), jnp.bfloat16).at[source, target].set(scaled_slots)
    results = lax.map(expert_pass, (to_experts(rows_in), to_experts(rows_scaled), gate_weight, up_weight, down_weight))
    slot_grad, score, gate_grad, up_grad, down_grad, gate_norm, up_norm, down_norm = results
    returned = to_blocks(slot_grad)
    per_slot = jnp.take_along_axis(returned, target[:, :, None], axis=1)
    per_slot = per_slot.astype(jnp.float32).reshape(N_EP * TOK_DEV, TOP_K, D)
    token_grad = jnp.sum(per_slot, axis=1).astype(jnp.bfloat16)
    score_back = jnp.take_along_axis(to_blocks(score), target, axis=1).reshape(N_EP * TOK_DEV, TOP_K)
    slot_score = score_back / weight
    expert_prob_grad = group_prob[:, None] * slot_score
    group_prob_grad = jnp.sum(expert_prob * slot_score, axis=1)
    return (token_grad, group_prob_grad, expert_prob_grad, gate_grad, up_grad, down_grad,
            gate_norm, up_norm, down_norm)
```

```python
import functools
import jax
import jax.numpy as jnp
from jax import lax
from jax.experimental import pallas as pl
from jax.experimental.pallas import tpu as pltpu
from jax.sharding import PartitionSpec as P

MESH = pl.DeviceIdType.MESH
CHUNKS = 8
DIRECT = 5


def dispatch_kernel(n_ep, mine_ref, out_ref, local_sem, send_sem, recv_sem, fwd_send, fwd_recv, z_send, z_recv):
    me = lax.axis_index("ep")
    t = lax.axis_index("tp")
    core = lax.rem(t, 2)
    partner = t + 1 - 2 * core
    side_z = lax.rem(t // 2, 2)
    across = t + 2 - 4 * side_z
    width = mine_ref.shape[2] // CHUNKS
    barrier = pltpu.get_barrier_semaphore()
    for d in range(1, n_ep):
        pl.semaphore_signal(
            barrier, inc=1, device_id={"ep": lax.rem(me + d, n_ep)}, device_id_type=MESH
        )
    pl.semaphore_signal(barrier, inc=1, device_id={"tp": partner}, device_id_type=MESH)
    pl.semaphore_signal(barrier, inc=1, device_id={"tp": across}, device_id_type=MESH)
    pl.semaphore_wait(barrier, n_ep + 1)

    def cols(c):
        j, side = (c, side_z) if c < DIRECT else (c - DIRECT, 1 - side_z)
        at = j + side * (CHUNKS - 1 - 2 * j)
        return pl.ds(pl.multiple_of(at * width, 128), width)

    def to_peer(d, c):
        dst = lax.rem(me + d, n_ep)
        return pltpu.make_async_remote_copy(
            src_ref=mine_ref.at[dst, :, cols(c)],
            dst_ref=out_ref.at[core, me, :, cols(c)],
            send_sem=send_sem.at[d, c],
            recv_sem=recv_sem.at[d, c],
            device_id={"ep": dst},
            device_id_type=MESH,
        )

    def from_peer(d, c):
        src = lax.rem(me - d + n_ep, n_ep)
        return pltpu.make_async_remote_copy(
            src_ref=mine_ref.at[me, :, cols(c)],
            dst_ref=out_ref.at[core, src, :, cols(c)],
            send_sem=send_sem.at[d, c],
            recv_sem=recv_sem.at[d, c],
            device_id={"ep": src},
            device_id_type=MESH,
        )

    def forward(d, c, side):
        src = lax.rem(me - d + n_ep, n_ep)
        source = mine_ref.at[me, :, cols(c)] if d == 0 else out_ref.at[side, src, :, cols(c)]
        return pltpu.make_async_remote_copy(
            src_ref=source,
            dst_ref=out_ref.at[side, src, :, cols(c)],
            send_sem=fwd_send.at[d, c],
            recv_sem=fwd_recv.at[d, c],
            device_id={"tp": partner},
            device_id_type=MESH,
        )

    def swap(d, c, arriving):
        src = lax.rem(me - d + n_ep, n_ep)
        ref = out_ref.at[core, src, :, cols(c + DIRECT if arriving else c)]
        return pltpu.make_async_remote_copy(
            src_ref=ref,
            dst_ref=ref,
            send_sem=z_send.at[d, c],
            recv_sem=z_recv.at[d, c],
            device_id={"tp": across},
            device_id_type=MESH,
        )

    order = sorted(range(1, n_ep), key=lambda d: abs(d - n_ep // 2))
    extra = CHUNKS - DIRECT
    for c in range(DIRECT):
        for d in order:
            to_peer(d, c).start()
    keep = pltpu.make_async_copy(mine_ref.at[me], out_ref.at[core, me], local_sem)
    keep.start()
    for c in range(CHUNKS):
        forward(0, c, core).start()
    lag = DIRECT - extra
    for c in range(DIRECT):
        for d in order:
            from_peer(d, c).wait_recv()
            if c < extra:
                swap(d, c, False).start()
            forward(d, c, core).start()
        if c >= lag:
            for d in order:
                swap(d, c - lag, True).wait_recv()
                forward(d, c - lag + DIRECT, core).start()
    keep.wait()
    for c in range(DIRECT):
        for d in order:
            to_peer(d, c).wait_send()
    for c in range(extra):
        for d in order:
            swap(d, c, False).wait_send()
    for d in range(n_ep):
        for c in range(CHUNKS):
            forward(d, c, core).wait_send()
            forward(d, c, 1 - core).wait_recv()


def dispatch(mine, n_ep):
    return pl.pallas_call(
        functools.partial(dispatch_kernel, n_ep),
        out_shape=jax.ShapeDtypeStruct((2,) + mine.shape, mine.dtype),
        in_specs=[pl.BlockSpec(memory_space=pltpu.VMEM)],
        out_specs=pl.BlockSpec(memory_space=pl.ANY),
        scratch_shapes=[
            pltpu.SemaphoreType.DMA,
            pltpu.SemaphoreType.DMA((n_ep, CHUNKS)),
            pltpu.SemaphoreType.DMA((n_ep, CHUNKS)),
            pltpu.SemaphoreType.DMA((n_ep, CHUNKS)),
            pltpu.SemaphoreType.DMA((n_ep, CHUNKS)),
            pltpu.SemaphoreType.DMA((n_ep, CHUNKS)),
            pltpu.SemaphoreType.DMA((n_ep, CHUNKS)),
        ],
        compiler_params=pltpu.CompilerParams(collective_id=0, has_side_effects=True),
        name="dispatch",
    )(mine)


def sums_kernel(n_ep, n_tp, part_ref, norm_ref, score_ref, slots, total, send_sem, recv_sem, s_send, s_recv):
    me = lax.axis_index("ep")
    t = lax.axis_index("tp")
    barrier = pltpu.get_barrier_semaphore()
    for d in range(1, n_tp):
        pl.semaphore_signal(
            barrier, inc=1, device_id={"tp": lax.rem(t + d, n_tp)}, device_id_type=MESH
        )
    for d in range(1, n_ep):
        pl.semaphore_signal(
            barrier, inc=1, device_id={"ep": lax.rem(me + d, n_ep)}, device_id_type=MESH
        )
    pl.semaphore_wait(barrier, n_tp - 1 + n_ep - 1)

    def part_to(d):
        return pltpu.make_async_remote_copy(
            src_ref=part_ref,
            dst_ref=slots.at[t],
            send_sem=send_sem.at[d],
            recv_sem=recv_sem.at[d],
            device_id={"tp": lax.rem(t + d, n_tp)},
            device_id_type=MESH,
        )

    def part_from(d):
        src = lax.rem(t - d + n_tp, n_tp)
        return pltpu.make_async_remote_copy(
            src_ref=part_ref,
            dst_ref=slots.at[src],
            send_sem=send_sem.at[d],
            recv_sem=recv_sem.at[d],
            device_id={"tp": src},
            device_id_type=MESH,
        )

    for d in range(1, n_tp):
        part_to(d).start()
    slots[t] = part_ref[...]
    for d in range(1, n_tp):
        part_from(d).wait_recv()
    acc = slots[0]
    for i in range(1, n_tp):
        acc = acc + slots[i]
    total[...] = acc
    rows = 8 * n_ep

    def score_to(d):
        dst = lax.rem(me + d, n_ep)
        return pltpu.make_async_remote_copy(
            src_ref=total.at[pl.ds(pl.multiple_of(dst * 8, 8), 8)],
            dst_ref=score_ref.at[me],
            send_sem=s_send.at[d],
            recv_sem=s_recv.at[d],
            device_id={"ep": dst},
            device_id_type=MESH,
        )

    def score_from(d):
        src = lax.rem(me - d + n_ep, n_ep)
        return pltpu.make_async_remote_copy(
            src_ref=total.at[pl.ds(0, 8)],
            dst_ref=score_ref.at[src],
            send_sem=s_send.at[d],
            recv_sem=s_recv.at[d],
            device_id={"ep": src},
            device_id_type=MESH,
        )

    norm_ref[...] = acc[rows:]
    for d in range(1, n_tp):
        part_to(d).wait_send()
    for d in range(1, n_ep):
        score_to(d).start()
    score_ref[me] = total[pl.ds(pl.multiple_of(me * 8, 8), 8)]
    for d in range(1, n_ep):
        score_from(d).wait_recv()
    for d in range(1, n_ep):
        score_to(d).wait_send()


def small_sums(scores, norms, n_ep, n_tp):
    cap = scores.shape[1]
    width = norms.shape[1]
    padded = jnp.pad(scores, ((0, 0), (0, 1024 - cap))).reshape(n_ep * 8, 128)
    part = jnp.concatenate([padded, norms.reshape(2 * width // 128, 128)], axis=0)
    norm_out, score_out = pl.pallas_call(
        functools.partial(sums_kernel, n_ep, n_tp),
        out_shape=(
            jax.ShapeDtypeStruct((2 * width // 128, 128), jnp.float32),
            jax.ShapeDtypeStruct((n_ep, 8, 128), jnp.float32),
        ),
        in_specs=[pl.BlockSpec(memory_space=pltpu.VMEM)],
        out_specs=(
            pl.BlockSpec(memory_space=pltpu.VMEM),
            pl.BlockSpec(memory_space=pltpu.VMEM),
        ),
        scratch_shapes=[
            pltpu.VMEM((n_tp,) + part.shape, jnp.float32),
            pltpu.VMEM(part.shape, jnp.float32),
            pltpu.SemaphoreType.DMA((n_tp,)),
            pltpu.SemaphoreType.DMA((n_tp,)),
            pltpu.SemaphoreType.DMA((n_ep,)),
            pltpu.SemaphoreType.DMA((n_ep,)),
        ],
        compiler_params=pltpu.CompilerParams(collective_id=1, has_side_effects=True),
        cost_estimate=pl.CostEstimate(flops=0, bytes_accessed=20_000_000, transcendentals=0),
        name="small_sums",
    )(part)
    return score_out.reshape(n_ep, 1024)[:, :cap], norm_out.reshape(2, width)


def fused_kernel(
    n_ep, n_tp, cap, tok_ref, cot_ref, gate_ref, up_ref, down_ref, route_hbm, group_hbm, prob_hbm,
    token_out, gate_g, up_g, down_g, gate_norm, up_norm, down_norm, prob_grad, group_grad,
    route_ref, group_ref, prob_ref, src_v, gate_v, up_v, down_v, mine, rows, gate_p, up_p, hid_p, pick_v, pick_t,
    part_out, part_in, part_own, part_sum, returned,
    tok_f, tok_b, a_in, b_out, b_in,
    norm_part, norm_in, norm_z, norm_fin, score_part, score_in, score_z, score_tot, score_ep,
    load_sem, sx, rx, zs, zr, fs, fr, ps, pr, es, er, a_s, a_r, b_s, b_r, c_s, c_r, e_s, e_r, q_s, q_r,
    f_s, f_r, ns, nr, nzs, nzr, nfs, nfr, ss, sr, szs, szr, ses, ser,
):
    bf, f32 = jnp.bfloat16, jnp.float32
    me = lax.axis_index("ep")
    t = lax.axis_index("tp")
    core = lax.rem(t, 2)
    z = t // 2
    nz = n_tp // 2
    side = lax.rem(z, 2)
    partner = t + 1 - 2 * core
    across = t + 2 - 4 * side
    middle = jnp.logical_and(z > 0, z < nz - 1)
    end = jnp.logical_or(z == 0, z == nz - 1)
    tok, width = token_out.shape
    ff = gate_v.shape[1]
    half = width // 2
    mid_peer = lax.rem(t + 2 * (3 - 2 * z) + n_tp, n_tp)
    peers = {1: me + 1 - 2 * lax.rem(me, 2), 2: lax.rem(me + 2, n_ep), 3: n_ep - 1 - me}

    def remote(src, dst, send, recv, device):
        return pltpu.make_async_remote_copy(
            src_ref=src, dst_ref=dst, send_sem=send, recv_sem=recv,
            device_id=device, device_id_type=MESH,
        )

    @pl.when(core == 0)
    def _():
        pltpu.make_async_copy(tok_ref, src_v, load_sem.at[0]).start()

    @pl.when(core == 1)
    def _():
        pltpu.make_async_copy(cot_ref, src_v, load_sem.at[0]).start()

    small = [
        pltpu.make_async_copy(a, b, load_sem.at[n + 4])
        for n, (a, b) in enumerate(
            ((route_hbm, route_ref), (group_hbm, group_ref), (prob_hbm, prob_ref))
        )
    ]
    for copy in small:
        copy.start()
    loads = [
        pltpu.make_async_copy(a, b, load_sem.at[n + 1])
        for n, (a, b) in enumerate(((gate_ref, gate_v), (up_ref, up_v), (down_ref, down_v)))
    ]
    for copy in loads:
        copy.start()

    barrier = pltpu.get_barrier_semaphore()
    for d in range(1, n_ep):
        pl.semaphore_signal(barrier, inc=1, device_id={"ep": peers[d]}, device_id_type=MESH)
    for d in range(1, nz):
        pl.semaphore_signal(
            barrier, inc=1, device_id={"tp": lax.rem(t + 2 * d, n_tp)}, device_id_type=MESH
        )
    pl.semaphore_signal(barrier, inc=1, device_id={"tp": partner}, device_id_type=MESH)

    for copy in small:
        copy.wait()
    order = [1, 2, 3, 0]
    first, second = route_ref[0:1, :], route_ref[1:2, :]
    weight = group_ref[...] * prob_ref[...]
    w0, w1 = weight[0:1, :], weight[1:2, :]
    experts = [me if d == 0 else peers[d] for d in range(n_ep)]
    hit0 = [first == e for e in experts]
    hit1 = [second == e for e in experts]
    named = [jnp.where(jnp.logical_or(x, y), 1.0, 0.0) for x, y in zip(hit0, hit1)]
    weight_of = [jnp.where(x, w0, 0.0) + jnp.where(y, w1, 0.0) for x, y in zip(hit0, hit1)]
    named8 = jnp.concatenate(named + [jnp.zeros((8 - n_ep, tok), f32)], axis=0)
    earlier = jnp.where(
        lax.broadcasted_iota(jnp.int32, (tok, tok), 0) < lax.broadcasted_iota(jnp.int32, (tok, tok), 1),
        1.0, 0.0,
    ).astype(bf)
    before = jnp.dot(named8.astype(bf), earlier, preferred_element_type=f32)
    place = jnp.where(named8 > 0.5, before, -1.0)
    slot = lax.broadcasted_iota(jnp.int32, (cap, tok), 0).astype(f32)
    is_cot = core.astype(f32)
    with jax.named_scope("w_src"):
        pltpu.make_async_copy(tok_ref, src_v, load_sem.at[0]).wait()

    sizes = [cap // 6, cap // 6, cap // 3]
    starts = [0, cap // 6, cap // 3]

    def span(c, s):
        at = starts[c] + s * (cap - 2 * starts[c] - sizes[c])
        return pl.multiple_of(at, 16), sizes[c]

    def block_rows(d, c, s):
        at, n = span(c, s)
        return pl.ds(pl.multiple_of(d * cap + at, 16), n)

    def to_peer(d, c):
        at, n = span(c, side)
        return remote(
            mine.at[d - 1, pl.ds(at, n)], rows.at[core, block_rows(d, c, side)],
            sx.at[d, c], rx.at[d, c], {"ep": peers[d]},
        )

    def swap(d, c, arriving):
        at = block_rows(d, c, 1 - side if arriving else side)
        ref = rows.at[core, at]
        return remote(ref, ref, zs.at[d, c], zr.at[d, c], {"tp": across})

    def share(d, c, swapped, kind):
        if d == 0:
            at = pl.ds(0, cap)
        else:
            at = block_rows(d, c, 1 - side if swapped else side)
        ref = rows.at[kind, at]
        n = c + 3 * swapped
        return remote(ref, ref, fs.at[d, n], fr.at[d, n], {"tp": partner})

    pieces = [(d, c, s) for d in range(1, n_ep) for c, s in ((0, 0), (1, 0), (2, 0), (0, 1), (1, 1))]

    greeted = False
    for d in order:
        with jax.named_scope("mine"):
            pick = jnp.where(slot == place[d:d + 1, :], 1.0, 0.0)
            pick_v[d] = pick.astype(bf)
            slot_weight = jnp.sum(pick * weight_of[d], axis=1, keepdims=True)
            factor = slot_weight * is_cot + (1.0 - is_cot)
            for n in range(0, width, 512):
                got = jnp.dot(pick_v[d], src_v[:, n:n + 512], preferred_element_type=f32)
                got = (got * factor).astype(bf)
                if d == 0:
                    rows[core, 0:cap, n:n + 512] = got
                else:
                    mine[d - 1, :, n:n + 512] = got
            if not greeted:
                with jax.named_scope("barrier"):
                    pl.semaphore_wait(barrier, n_ep - 1 + nz)
                greeted = True
            if d == 0:
                share(0, 0, 0, core).start()
            elif d == 3:
                for e, c in ((3, 0), (1, 2), (2, 2), (3, 1), (3, 2)):
                    to_peer(e, c).start()
            else:
                for c in (0, 1):
                    to_peer(d, c).start()

    column = jnp.transpose(place)
    lane = lax.broadcasted_iota(jnp.int32, (tok, cap), 1).astype(f32)
    for d in range(n_ep):
        pick_t[d] = jnp.where(lane == column[:, d:d + 1], 1.0, 0.0).astype(bf)

    last = (((1,), (1,)), ((), ()))
    contract = (((0,), (0,)), ((), ()))

    def fold(sq):
        parts = [sq[:, j * 128:(j + 1) * 128] for j in range(sq.shape[1] // 128)]
        return functools.reduce(jnp.add, parts)

    mine_half = pl.multiple_of(core * half, 128)
    other_half = pl.multiple_of((1 - core) * half, 128)

    def exchange(lo, n):
        at = pl.ds(lo * cap, n * cap)
        return remote(part_out.at[at], part_in.at[at], ps.at[lo], pr.at[lo], {"tp": partner})

    jw = 128
    steps = half // jw
    groups = ((0, 1), (1, 2), (3, 1))

    def back(d, j):
        w = jw if d == 3 else half // 2
        at = pl.ds(j * w, w)
        return remote(
            part_sum.at[d - 1, :, at], returned.at[d, :, at], es.at[d, j], er.at[d, j], {"ep": peers[d]}
        )

    def block(lo, count, between=()):
        at = slice(lo * cap, (lo + count) * cap)
        score = None
        for n in range(0, ff, 256):
            with jax.named_scope("fwd"):
                pre_gate = jnp.dot(rows[0, at, :], gate_v[:, n:n + 256], preferred_element_type=f32)
                pre_up = jnp.dot(rows[0, at, :], up_v[:, n:n + 256], preferred_element_type=f32)
                grad = lax.dot_general(rows[1, at, :], down_v[n:n + 256, :], last, preferred_element_type=f32)
                sigma = jax.nn.sigmoid(pre_gate)
                activated = pre_gate * sigma
                derivative = sigma * (1.0 + pre_gate * (1.0 - sigma))
                hidden = (activated * pre_up).astype(bf)
                hid_p[at, n:n + 256] = hidden
                more = fold(hidden.astype(f32) * grad)
                score = more if score is None else score + more
                gate_p[at, n:n + 256] = (grad * pre_up * derivative).astype(bf)
                up_p[at, n:n + 256] = (grad * activated).astype(bf)
        for i in range(count):
            score_part[lo + i:lo + i + 1, 0:cap] = jnp.sum(
                jnp.transpose(score[i * cap:(i + 1) * cap]), axis=0, keepdims=True
            )

        def part(c):
            got = lax.dot_general(gate_p[at, :], gate_v[pl.ds(c, 256), :], last, preferred_element_type=f32)
            return got + lax.dot_general(
                up_p[at, :], up_v[pl.ds(c, 256), :], last, preferred_element_type=f32
            )

        with jax.named_scope("part_other"):
            for n in range(0, half, 256):
                part_out[at, n:n + 256] = part(pl.multiple_of(other_half + n, 128)).astype(bf)
        exchange(lo, count).start()
        for step in between:
            step()
        with jax.named_scope("part_own"):
            for n in range(0, half, 256):
                part_own[0:count * cap, n:n + 256] = part(pl.multiple_of(mine_half + n, 128))
        with jax.named_scope("w_part"):
            exchange(lo, count).wait_recv()
        for n in range(0, half, 256):
            total = part_own[0:count * cap, n:n + 256] + part_in[at, n:n + 256].astype(f32)
            total = total.astype(bf)
            for i in range(count):
                piece = total[i * cap:(i + 1) * cap]
                if lo == 0:
                    returned[0, :, n:n + 256] = piece
                else:
                    part_sum[lo + i - 1, :, n:n + 256] = piece
        if lo == 3:
            for j in range(steps // 2):
                back(3, j).start()
            back(1, 1).start()
            back(2, 1).start()
            for j in range(steps // 2, steps):
                back(3, j).start()
        elif lo:
            back(1, 0).start()
            back(2, 0).start()

    def arrive(d, c):
        to_peer(d, c).wait_recv()
        if c < 2:
            swap(d, c, False).start()
        share(d, c, 0, core).start()

    def arrive_swap(d, c):
        swap(d, c, True).wait_recv()
        share(d, c, 1, core).start()

    def shared(d):
        for c, s in ((0, 0), (1, 0), (2, 0), (0, 1), (1, 1)):
            share(d, c, s, 1 - core).wait_recv()

    score_part[...] = jnp.zeros_like(score_part)
    with jax.named_scope("w_own"):
        share(0, 0, 0, 1 - core).wait_recv()
        for copy in loads:
            copy.wait()
    block(0, 1, (lambda: arrive(1, 0), lambda: arrive(2, 0)))
    with jax.named_scope("w_1"):
        arrive(1, 1)
        arrive(2, 1)
    with jax.named_scope("w_g0"):
        arrive(3, 0)
    with jax.named_scope("w_swap0"):
        arrive_swap(1, 0)
        arrive_swap(2, 0)
    with jax.named_scope("w_2"):
        arrive(1, 2)
        arrive(2, 2)
    with jax.named_scope("w_swap1"):
        arrive_swap(1, 1)
        arrive_swap(2, 1)
    with jax.named_scope("w_sh12"):
        shared(1)
        shared(2)
    block(1, 2, (lambda: arrive(3, 1),))
    with jax.named_scope("w_gswap0"):
        arrive_swap(3, 0)
    with jax.named_scope("w_g2"):
        arrive(3, 2)
    with jax.named_scope("w_gswap1"):
        arrive_swap(3, 1)
    with jax.named_scope("w_gsh"):
        shared(3)
    block(3, 1)

    def score_pair():
        return remote(score_part, score_in, ss, sr, {"tp": partner})

    def score_to(d):
        return remote(score_tot, score_z.at[z], szs.at[d], szr.at[d], {"tp": lax.rem(t + 2 * d, n_tp)})

    def score_from(d):
        src = lax.rem(z - d + nz, nz)
        return remote(
            score_tot, score_z.at[src], szs.at[d], szr.at[d], {"tp": lax.rem(t - 2 * d + n_tp, n_tp)}
        )

    def score_back(d):
        return remote(score_fin, score_ep.at[d], ses.at[d], ser.at[d], {"ep": peers[d]})

    score_fin = score_in
    score_pair().start()

    def gate_up(k):
        at = pl.ds(pl.multiple_of(k * 256, 256), 256)
        lhs = rows[0, :, at]
        for n, (rhs, out) in enumerate(((gate_p, gate_g), (up_p, up_g))):
            total = lax.dot_general(lhs, rhs[...], contract, preferred_element_type=f32)
            out[at, :] = total.astype(bf)
            sq = fold(total * total)
            for h in range(2):
                norm_part[n, pl.ds(k * 2 + h, 1), :] = jnp.sum(
                    jnp.transpose(sq[h * 128:(h + 1) * 128]), axis=0, keepdims=True
                ) / (ff * n_tp)

    def loop_gate_up(lo, hi):
        def body(k, carry):
            gate_up(k)
            return carry
        lax.fori_loop(lo, hi, body, 0)

    def down(k):
        at = pl.ds(pl.multiple_of(k * 256, 256), 256)
        lhs = hid_p[:, at]
        sq = None
        for c in range(0, width, 512):
            total = lax.dot_general(lhs, rows[1, :, c:c + 512], contract, preferred_element_type=f32)
            down_g[at, c:c + 512] = total.astype(bf)
            more = fold(total * total)
            sq = more if sq is None else sq + more
        for h in range(2):
            down_norm[0:1, k * 256 + h * 128:k * 256 + (h + 1) * 128] = jnp.sum(
                jnp.transpose(sq[h * 128:(h + 1) * 128]), axis=0, keepdims=True
            ) / width

    def norm_pair():
        return remote(norm_part.at[1 - core], norm_in, ns, nr, {"tp": partner})

    def norm_to(d):
        return remote(norm_part.at[core], norm_z.at[z], nzs.at[d], nzr.at[d],
                      {"tp": lax.rem(t + 2 * d, n_tp)})

    def norm_from(d):
        src = lax.rem(z - d + nz, nz)
        return remote(norm_part.at[core], norm_z.at[src], nzs.at[d], nzr.at[d],
                      {"tp": lax.rem(t - 2 * d + n_tp, n_tp)})

    def norm_done(kind):
        ref = norm_fin.at[kind]
        return remote(ref, ref, nfs, nfr, {"tp": partner})

    def work_score_a():
        score_pair().wait_recv()
        score_pair().wait_send()
        score_tot[...] = score_part[...] + score_in[...]
        for d in range(1, nz):
            score_to(d).start()
        score_z[z] = score_tot[...]

    def work_norm_a():
        norm_pair().start()

    def work_norm_b():
        norm_pair().wait_recv()
        norm_pair().wait_send()
        norm_part[core] = norm_part[core] + norm_in[...]
        for d in range(1, nz):
            norm_to(d).start()
        norm_z[z] = norm_part[core]

    def work_score_b():
        for d in range(1, nz):
            score_from(d).wait_recv()
        score_fin[...] = functools.reduce(jnp.add, [score_z[i] for i in range(nz)])
        for d in range(1, n_ep):
            score_back(d).start()

    def work_norm_c():
        for d in range(1, nz):
            norm_from(d).wait_recv()
        norm_fin[core] = functools.reduce(jnp.add, [norm_z[i] for i in range(nz)])
        norm_done(core).start()

    def work_score_c():
        of0 = jnp.zeros((1, tok), f32)
        of1 = jnp.zeros((1, tok), f32)
        for d in range(n_ep):
            if d:
                score_back(d).wait_recv()
            line = score_fin if d == 0 else score_ep.at[d]
            hit = jnp.dot(
                line[:, 0:cap], pick_v[d].astype(f32), preferred_element_type=f32,
                precision=lax.Precision.HIGHEST,
            )
            hit = hit[d:d + 1, :]
            of0 = of0 + jnp.where(hit0[d], hit, 0.0)
            of1 = of1 + jnp.where(hit1[d], hit, 0.0)
        slot0, slot1 = of0 / w0, of1 / w1
        prob_grad[0:1, :] = group_ref[...] * slot0
        prob_grad[1:2, :] = group_ref[...] * slot1
        group_grad[...] = prob_ref[0:1, :] * slot0 + prob_ref[1:2, :] * slot1

    def work_norm_d():
        norm_done(1 - core).wait_recv()
        for i in range(width // 128):
            gate_norm[0:1, i * 128:(i + 1) * 128] = norm_fin[0, i:i + 1, :]
            up_norm[0:1, i * 128:(i + 1) * 128] = norm_fin[1, i:i + 1, :]

    strips = width // 256
    with jax.named_scope("gate_up"):
        loop_gate_up(0, strips // 2)
    with jax.named_scope("score_a"):
        work_score_a()

    th = tok // 2
    own_at = pl.multiple_of((z - 1) * th, 128)
    far_at = pl.multiple_of((2 - z) * th, 128)

    def cols(c, j):
        return pl.ds(pl.multiple_of(c * half + j * jw, 128), jw)

    def a_copy(j):
        return remote(tok_b.at[j], a_in.at[j], a_s.at[j], a_r.at[j], {"tp": across})

    def b_copy(j):
        return remote(b_out.at[j], b_in.at[j], b_s.at[j], b_r.at[j], {"tp": mid_peer})

    def c_copy(j, at):
        ref = token_out.at[pl.ds(at, th), cols(core, j)]
        return remote(ref, ref, c_s.at[j], c_r.at[j], {"tp": mid_peer})

    def e_copy(j, at):
        ref = token_out.at[pl.ds(at, th), cols(core, j)]
        return remote(ref, ref, e_s.at[j], e_r.at[j], {"tp": across})

    def q_copy(j, at):
        ref = token_out.at[pl.ds(at, th), cols(core, j)]
        return remote(ref, ref, q_s.at[j], q_r.at[j], {"tp": across})

    def f_copy(j, c):
        ref = token_out.at[:, cols(c, j)]
        return remote(ref, ref, f_s.at[j], f_r.at[j], {"tp": partner})

    near_at = pl.multiple_of(jnp.where(z == 0, 0, th), 128)
    beyond_at = pl.multiple_of(jnp.where(z == 0, th, 0), 128)

    lag_a, lag_b, lag_c, lag_e = 1, 3, 5, steps

    def combine(j):
        if j % (steps // 2) == 0:
            back(1, 2 * j // steps).wait_recv()
            back(2, 2 * j // steps).wait_recv()
        back(3, j).wait_recv()
        at = slice(j * jw, (j + 1) * jw)
        total = None
        for d in range(n_ep):
            more = jnp.dot(pick_t[d], returned[d, :, at], preferred_element_type=f32)
            total = more if total is None else total + more

        @pl.when(end)
        def _():
            tok_b[j] = total.astype(bf)
            a_copy(j).start()

        @pl.when(middle)
        def _():
            tok_f[j] = total

    def pair_sum(j):
        @pl.when(middle)
        def _():
            a_copy(j).wait_recv()
            b_out[j] = (
                tok_f[j, pl.ds(far_at, th), :] + a_in[j, pl.ds(far_at, th), :].astype(f32)
            ).astype(bf)
            b_copy(j).start()
            tok_f[j, pl.ds(own_at, th), :] = (
                tok_f[j, pl.ds(own_at, th), :] + a_in[j, pl.ds(own_at, th), :].astype(f32)
            )

    def line_sum(j):
        @pl.when(middle)
        def _():
            b_copy(j).wait_recv()
            token_out[pl.ds(own_at, th), cols(core, j)] = (
                tok_f[j, pl.ds(own_at, th), :] + b_in[j].astype(f32)
            ).astype(bf)
            c_copy(j, own_at).start()
            e_copy(j, own_at).start()

    def relay(j):
        @pl.when(middle)
        def _():
            c_copy(j, far_at).wait_recv()
            q_copy(j, far_at).start()
            f_copy(j, core).start()

    def collect(j):
        @pl.when(end)
        def _():
            e_copy(j, near_at).wait_recv()
            q_copy(j, beyond_at).wait_recv()
            f_copy(j, core).start()

    left = strips - strips // 2
    filler = {
        i: [lambda i=i: loop_gate_up(strips // 2 + i * left // 3, strips // 2 + (i + 1) * left // 3)]
        for i in range(3)
    }
    filler[1].append(work_score_b)
    filler[3] = [work_norm_a, lambda: down(0)]
    filler[4] = [work_norm_b]
    filler[5] = [lambda: down(1)]
    stages = (
        ("combine", 0, combine), ("pair_sum", lag_a, pair_sum), ("line_sum", lag_b, line_sum),
        ("relay", lag_c, relay), ("collect", lag_e, collect),
    )
    for s in range(steps + lag_e):
        for name, lag, step in stages:
            if 0 <= s - lag < steps:
                with jax.named_scope(name):
                    step(s - lag)
        for item in filler.get(s, []):
            with jax.named_scope("filler"):
                item()

    with jax.named_scope("last"):
        work_score_c()
        work_norm_c()
        work_norm_d()

    with jax.named_scope("w_final"):
        for j in range(steps):
            f_copy(j, 1 - core).wait_recv()
            f_copy(j, core).wait_send()
            back(3, j).wait_send()

    @pl.when(end)
    def _():
        for j in range(steps):
            a_copy(j).wait_send()

    @pl.when(middle)
    def _():
        for j in range(steps):
            b_copy(j).wait_send()
            c_copy(j, own_at).wait_send()
            e_copy(j, own_at).wait_send()
            q_copy(j, far_at).wait_send()

    for lo, n in groups:
        exchange(lo, n).wait_send()
    for d in (1, 2):
        back(d, 0).wait_send()
        back(d, 1).wait_send()
    share(0, 0, 0, core).wait_send()
    for d, c, s in pieces:
        share(d, c, s, core).wait_send()
        if not s:
            to_peer(d, c).wait_send()
            if c < 2:
                swap(d, c, False).wait_send()
    for d in range(1, nz):
        score_to(d).wait_send()
        norm_to(d).wait_send()
    for d in range(1, n_ep):
        score_back(d).wait_send()
    norm_done(core).wait_send()


def store_kernel(count, *refs):
    sem = refs[-1]
    copies = [pltpu.make_async_copy(refs[n], refs[count + n], sem.at[n]) for n in range(count)]
    for copy in copies:
        copy.start()
    for copy in copies:
        copy.wait()


def fused(tokens, cotangent, group_prob, expert_prob, routing, gate_weight, up_weight, down_weight):
    tok, width = tokens.shape
    n_ep = lax.axis_size("ep")
    n_tp = lax.axis_size("tp")
    ff = gate_weight.shape[2]
    cap = 3 * tok * routing.shape[1] // (2 * n_ep)
    slots = n_ep * cap
    nz = n_tp // 2
    half = width // 2
    jw = 128
    steps = half // jw
    th = tok // 2
    bf, f32 = jnp.bfloat16, jnp.float32
    vm = pltpu.VMEM
    dma = pltpu.SemaphoreType.DMA
    vmem = pl.BlockSpec(memory_space=pltpu.VMEM)
    hbm = pl.BlockSpec(memory_space=pl.ANY)
    shapes = (
        jax.ShapeDtypeStruct((tok, width), bf),
        jax.ShapeDtypeStruct((width, ff), bf),
        jax.ShapeDtypeStruct((width, ff), bf),
        jax.ShapeDtypeStruct((ff, width), bf),
        jax.ShapeDtypeStruct((1, width), f32),
        jax.ShapeDtypeStruct((1, width), f32),
        jax.ShapeDtypeStruct((1, ff), f32),
        jax.ShapeDtypeStruct((2, tok), f32),
        jax.ShapeDtypeStruct((1, tok), f32),
    )
    count = len(shapes)
    outs = pl.pallas_call(
        functools.partial(fused_kernel, n_ep, n_tp, cap),
        out_shape=tuple(pltpu.VMEM(x.shape, x.dtype) for x in shapes),
        in_specs=[hbm] * 8,
        out_specs=(vmem,) * count,
        scratch_shapes=[
            vm((2, tok), jnp.int32), vm((1, tok), f32), vm((2, tok), f32),
            vm((tok, width), bf), vm((width, ff), bf), vm((width, ff), bf), vm((ff, width), bf),
            vm((n_ep - 1, cap, width), bf), vm((2, slots, width), bf),
            vm((slots, ff), bf), vm((slots, ff), bf), vm((slots, ff), bf),
            vm((n_ep, cap, tok), bf), vm((n_ep, tok, cap), bf),
            vm((slots, half), bf), vm((slots, half), bf), vm((2 * cap, half), f32),
            vm((n_ep - 1, cap, half), bf), vm((n_ep, cap, half), bf),
            vm((steps, tok, jw), f32), vm((steps, tok, jw), bf), vm((steps, tok, jw), bf),
            vm((steps, th, jw), bf), vm((steps, th, jw), bf),
            vm((2, width // 128, 128), f32), vm((width // 128, 128), f32),
            vm((nz, width // 128, 128), f32), vm((2, width // 128, 128), f32),
            vm((8, tok), f32), vm((8, tok), f32), vm((nz, 8, tok), f32), vm((8, tok), f32),
            vm((n_ep, 8, tok), f32),
            dma((7,)), dma((n_ep, 3)), dma((n_ep, 3)), dma((n_ep, 2)), dma((n_ep, 2)),
            dma((n_ep, 5)), dma((n_ep, 5)), dma((n_ep,)), dma((n_ep,)),
            dma((n_ep, steps)), dma((n_ep, steps)),
        ] + [dma((steps,))] * 12 + [
            dma, dma, dma((nz,)), dma((nz,)), dma, dma, dma, dma, dma((nz,)), dma((nz,)),
            dma((n_ep,)), dma((n_ep,)),
        ],
        compiler_params=pltpu.CompilerParams(
            collective_id=3, has_side_effects=True, vmem_limit_bytes=56 << 20
        ),
        name="fused",
    )(
        tokens, cotangent, gate_weight[0], up_weight[0], down_weight[0],
        routing.T, group_prob.reshape(1, tok), expert_prob.T,
    )
    outs = pl.pallas_call(
        functools.partial(store_kernel, count),
        out_shape=shapes,
        in_specs=[vmem] * count,
        out_specs=(hbm,) * count,
        scratch_shapes=[dma((count,))],
        compiler_params=pltpu.CompilerParams(vmem_limit_bytes=1 << 20),
        name="store",
    )(*outs)
    token_grad, gate_g, up_g, down_g, gate_n, up_n, down_n, prob_g, group_g = outs
    return (
        token_grad, group_g.reshape(tok), prob_g.T, gate_g[None], up_g[None], down_g[None],
        gate_n, up_n, down_n,
    )


def general(tokens, cotangent, group_prob, expert_prob, routing, gate_weight, up_weight, down_weight):
    tok_count, model_width = tokens.shape
    top_count = routing.shape[1]
    n_ep = lax.axis_size("ep")
    n_tp = lax.axis_size("tp")
    capacity = 3 * tok_count * top_count // (2 * n_ep)
    buffer_rows = n_ep * capacity
    core = lax.rem(lax.axis_index("tp"), 2)
    weight = group_prob[:, None] * expert_prob

    experts = jnp.arange(n_ep, dtype=jnp.int32)[:, None]
    picks = [routing[None, :, k] == experts for k in range(top_count)]
    named = functools.reduce(jnp.logical_or, picks)
    weight_of = sum(jnp.where(picks[k], weight[None, :, k], 0.0) for k in range(top_count))
    earlier = (
        lax.broadcasted_iota(jnp.int32, (tok_count, tok_count), 0)
        < lax.broadcasted_iota(jnp.int32, (tok_count, tok_count), 1)
    ).astype(jnp.bfloat16)
    before = jnp.dot(named.astype(jnp.bfloat16), earlier, preferred_element_type=jnp.float32)
    place = jnp.where(named, before.astype(jnp.int32), -1)
    filled = place[:, None, :] == lax.broadcasted_iota(jnp.int32, (n_ep, capacity, tok_count), 1)
    pick = filled.astype(jnp.bfloat16).reshape(buffer_rows, tok_count)
    slot_weight = jnp.sum(jnp.where(filled, weight_of[:, None, :], 0.0), axis=2).reshape(buffer_rows, 1)

    source = jnp.where(core == 0, tokens, cotangent)
    factor = jnp.where(core == 0, 1.0, slot_weight)
    mine = jnp.dot(pick, source, preferred_element_type=jnp.float32) * factor
    mine = mine.astype(jnp.bfloat16).reshape(n_ep, capacity, model_width)
    both = dispatch(mine, n_ep)
    flat_in = both[0].reshape(buffer_rows, model_width)
    flat_scaled = both[1].reshape(buffer_rows, model_width)

    w_gate = gate_weight[0]
    w_up = up_weight[0]
    w_down = down_weight[0]
    hidden_total = gate_weight.shape[2] * n_tp
    contract_last = (((1,), (1,)), ((), ()))
    contract_rows = (((0,), (0,)), ((), ()))
    pre_gate = jnp.dot(flat_in, w_gate, preferred_element_type=jnp.float32)
    pre_up = jnp.dot(flat_in, w_up, preferred_element_type=jnp.float32)
    sigma = jax.nn.sigmoid(pre_gate)
    activated = pre_gate * sigma
    derivative = sigma * (1.0 + pre_gate * (1.0 - sigma))
    hidden = (activated * pre_up).astype(jnp.bfloat16)
    hidden_grad = lax.dot_general(
        flat_scaled, w_down, contract_last, preferred_element_type=jnp.float32
    )
    score_part = jnp.sum(hidden.astype(jnp.float32) * hidden_grad, axis=1).reshape(n_ep, capacity)
    gate_pre = (hidden_grad * pre_up * derivative).astype(jnp.bfloat16)
    up_pre = (hidden_grad * activated).astype(jnp.bfloat16)
    input_part = lax.dot_general(
        gate_pre, w_gate, contract_last, preferred_element_type=jnp.float32
    )
    input_part = input_part + lax.dot_general(
        up_pre, w_up, contract_last, preferred_element_type=jnp.float32
    )
    input_part = input_part.astype(jnp.bfloat16).reshape(n_ep, capacity, model_width)
    share = lax.psum_scatter(input_part, "tp", scatter_dimension=2, tiled=True)

    down_sum = lax.dot_general(
        hidden, flat_scaled, contract_rows, preferred_element_type=jnp.float32
    )
    gate_sum = lax.dot_general(flat_in, gate_pre, contract_rows, preferred_element_type=jnp.float32)
    up_sum = lax.dot_general(flat_in, up_pre, contract_rows, preferred_element_type=jnp.float32)
    norm_part = (
        jnp.stack([jnp.sum(gate_sum * gate_sum, axis=1), jnp.sum(up_sum * up_sum, axis=1)])
        / hidden_total
    )
    down_norms = jnp.sum(down_sum * down_sum, axis=1) / model_width
    scores, row_norms = small_sums(score_part, norm_part, n_ep, n_tp)

    share, scores, row_norms, down_norms = lax.optimization_barrier(
        (share, scores, row_norms, down_norms)
    )
    returned = lax.all_to_all(share, "ep", split_axis=0, concat_axis=0, tiled=True)
    returned = returned.reshape(buffer_rows, -1)
    token_share = lax.dot_general(pick, returned, contract_rows, preferred_element_type=jnp.float32)
    token_grad = lax.all_gather(token_share.astype(jnp.bfloat16), "tp", axis=1, tiled=True)
    gate_grad, up_grad, down_grad = (
        x.astype(jnp.bfloat16) for x in (gate_sum, up_sum, down_sum)
    )


    score_of = jnp.sum(jnp.where(filled, scores[:, :, None], 0.0), axis=1)
    slot_score = jnp.stack(
        [jnp.sum(jnp.where(p, score_of, 0.0), axis=0) for p in picks], axis=1
    ) / weight
    expert_prob_grad = group_prob[:, None] * slot_score
    group_prob_grad = jnp.sum(expert_prob * slot_score, axis=1)
    return (
        token_grad,
        group_prob_grad,
        expert_prob_grad,
        gate_grad[None],
        up_grad[None],
        down_grad[None],
        row_norms[0][None],
        row_norms[1][None],
        down_norms[None],
    )


def local(*args):
    n_ep, n_tp = lax.axis_size("ep"), lax.axis_size("tp")
    tok, width = args[0].shape
    ff = args[5].shape[2]
    cap = 3 * tok * args[4].shape[1] // (2 * n_ep)
    fits = cap % 96 == 0 and tok % 256 == 0 and width % 2048 == 0 and ff % 256 == 0
    if n_ep == 4 and n_tp == 8 and args[4].shape[1] == 2 and fits:
        return fused(*args)
    return general(*args)


def solution(mesh):
    return jax.shard_map(
        local,
        mesh=mesh,
        in_specs=(
            P("ep", None),
            P("ep", None),
            P("ep"),
            P("ep", None),
            P("ep", None),
            P("ep", None, "tp"),
            P("ep", None, "tp"),
            P("ep", "tp", None),
        ),
        out_specs=(
            P("ep", None),
            P("ep"),
            P("ep", None),
            P("ep", None, "tp"),
            P("ep", None, "tp"),
            P("ep", "tp", None),
            P("ep", None),
            P("ep", None),
            P("ep", "tp"),
        ),
        check_vma=False,
    )
```

```python
import functools
import jax
import jax.numpy as jnp
from jax import lax
from jax.experimental import pallas as pl
from jax.experimental.pallas import tpu as pltpu
from jax.sharding import PartitionSpec as P

MESH = pl.DeviceIdType.MESH
CHUNKS = 8
DIRECT = 5


def dispatch_kernel(n_ep, mine_ref, out_ref, local_sem, send_sem, recv_sem, fwd_send, fwd_recv, z_send, z_recv):
    me = lax.axis_index("ep")
    t = lax.axis_index("tp")
    core = lax.rem(t, 2)
    partner = t + 1 - 2 * core
    side_z = lax.rem(t // 2, 2)
    across = t + 2 - 4 * side_z
    width = mine_ref.shape[2] // CHUNKS
    barrier = pltpu.get_barrier_semaphore()
    for d in range(1, n_ep):
        pl.semaphore_signal(
            barrier, inc=1, device_id={"ep": lax.rem(me + d, n_ep)}, device_id_type=MESH
        )
    pl.semaphore_signal(barrier, inc=1, device_id={"tp": partner}, device_id_type=MESH)
    pl.semaphore_signal(barrier, inc=1, device_id={"tp": across}, device_id_type=MESH)
    pl.semaphore_wait(barrier, n_ep + 1)

    def cols(c):
        j, side = (c, side_z) if c < DIRECT else (c - DIRECT, 1 - side_z)
        at = j + side * (CHUNKS - 1 - 2 * j)
        return pl.ds(pl.multiple_of(at * width, 128), width)

    def to_peer(d, c):
        dst = lax.rem(me + d, n_ep)
        return pltpu.make_async_remote_copy(
            src_ref=mine_ref.at[dst, :, cols(c)],
            dst_ref=out_ref.at[core, me, :, cols(c)],
            send_sem=send_sem.at[d, c],
            recv_sem=recv_sem.at[d, c],
            device_id={"ep": dst},
            device_id_type=MESH,
        )

    def from_peer(d, c):
        src = lax.rem(me - d + n_ep, n_ep)
        return pltpu.make_async_remote_copy(
            src_ref=mine_ref.at[me, :, cols(c)],
            dst_ref=out_ref.at[core, src, :, cols(c)],
            send_sem=send_sem.at[d, c],
            recv_sem=recv_sem.at[d, c],
            device_id={"ep": src},
            device_id_type=MESH,
        )

    def forward(d, c, side):
        src = lax.rem(me - d + n_ep, n_ep)
        source = mine_ref.at[me, :, cols(c)] if d == 0 else out_ref.at[side, src, :, cols(c)]
        return pltpu.make_async_remote_copy(
            src_ref=source,
            dst_ref=out_ref.at[side, src, :, cols(c)],
            send_sem=fwd_send.at[d, c],
            recv_sem=fwd_recv.at[d, c],
            device_id={"tp": partner},
            device_id_type=MESH,
        )

    def swap(d, c, arriving):
        src = lax.rem(me - d + n_ep, n_ep)
        ref = out_ref.at[core, src, :, cols(c + DIRECT if arriving else c)]
        return pltpu.make_async_remote_copy(
            src_ref=ref,
            dst_ref=ref,
            send_sem=z_send.at[d, c],
            recv_sem=z_recv.at[d, c],
            device_id={"tp": across},
            device_id_type=MESH,
        )

    order = sorted(range(1, n_ep), key=lambda d: abs(d - n_ep // 2))
    extra = CHUNKS - DIRECT
    for c in range(DIRECT):
        for d in order:
            to_peer(d, c).start()
    keep = pltpu.make_async_copy(mine_ref.at[me], out_ref.at[core, me], local_sem)
    keep.start()
    for c in range(CHUNKS):
        forward(0, c, core).start()
    lag = DIRECT - extra
    for c in range(DIRECT):
        for d in order:
            from_peer(d, c).wait_recv()
            if c < extra:
                swap(d, c, False).start()
            forward(d, c, core).start()
        if c >= lag:
            for d in order:
                swap(d, c - lag, True).wait_recv()
                forward(d, c - lag + DIRECT, core).start()
    keep.wait()
    for c in range(DIRECT):
        for d in order:
            to_peer(d, c).wait_send()
    for c in range(extra):
        for d in order:
            swap(d, c, False).wait_send()
    for d in range(n_ep):
        for c in range(CHUNKS):
            forward(d, c, core).wait_send()
            forward(d, c, 1 - core).wait_recv()


def dispatch(mine, n_ep):
    return pl.pallas_call(
        functools.partial(dispatch_kernel, n_ep),
        out_shape=jax.ShapeDtypeStruct((2,) + mine.shape, mine.dtype),
        in_specs=[pl.BlockSpec(memory_space=pltpu.VMEM)],
        out_specs=pl.BlockSpec(memory_space=pl.ANY),
        scratch_shapes=[
            pltpu.SemaphoreType.DMA,
            pltpu.SemaphoreType.DMA((n_ep, CHUNKS)),
            pltpu.SemaphoreType.DMA((n_ep, CHUNKS)),
            pltpu.SemaphoreType.DMA((n_ep, CHUNKS)),
            pltpu.SemaphoreType.DMA((n_ep, CHUNKS)),
            pltpu.SemaphoreType.DMA((n_ep, CHUNKS)),
            pltpu.SemaphoreType.DMA((n_ep, CHUNKS)),
        ],
        compiler_params=pltpu.CompilerParams(collective_id=0, has_side_effects=True),
        name="dispatch",
    )(mine)


def sums_kernel(n_ep, n_tp, part_ref, norm_ref, score_ref, slots, total, send_sem, recv_sem, s_send, s_recv):
    me = lax.axis_index("ep")
    t = lax.axis_index("tp")
    barrier = pltpu.get_barrier_semaphore()
    for d in range(1, n_tp):
        pl.semaphore_signal(
            barrier, inc=1, device_id={"tp": lax.rem(t + d, n_tp)}, device_id_type=MESH
        )
    for d in range(1, n_ep):
        pl.semaphore_signal(
            barrier, inc=1, device_id={"ep": lax.rem(me + d, n_ep)}, device_id_type=MESH
        )
    pl.semaphore_wait(barrier, n_tp - 1 + n_ep - 1)

    def part_to(d):
        return pltpu.make_async_remote_copy(
            src_ref=part_ref,
            dst_ref=slots.at[t],
            send_sem=send_sem.at[d],
            recv_sem=recv_sem.at[d],
            device_id={"tp": lax.rem(t + d, n_tp)},
            device_id_type=MESH,
        )

    def part_from(d):
        src = lax.rem(t - d + n_tp, n_tp)
        return pltpu.make_async_remote_copy(
            src_ref=part_ref,
            dst_ref=slots.at[src],
            send_sem=send_sem.at[d],
            recv_sem=recv_sem.at[d],
            device_id={"tp": src},
            device_id_type=MESH,
        )

    for d in range(1, n_tp):
        part_to(d).start()
    slots[t] = part_ref[...]
    for d in range(1, n_tp):
        part_from(d).wait_recv()
    acc = slots[0]
    for i in range(1, n_tp):
        acc = acc + slots[i]
    total[...] = acc
    rows = 8 * n_ep

    def score_to(d):
        dst = lax.rem(me + d, n_ep)
        return pltpu.make_async_remote_copy(
            src_ref=total.at[pl.ds(pl.multiple_of(dst * 8, 8), 8)],
            dst_ref=score_ref.at[me],
            send_sem=s_send.at[d],
            recv_sem=s_recv.at[d],
            device_id={"ep": dst},
            device_id_type=MESH,
        )

    def score_from(d):
        src = lax.rem(me - d + n_ep, n_ep)
        return pltpu.make_async_remote_copy(
            src_ref=total.at[pl.ds(0, 8)],
            dst_ref=score_ref.at[src],
            send_sem=s_send.at[d],
            recv_sem=s_recv.at[d],
            device_id={"ep": src},
            device_id_type=MESH,
        )

    norm_ref[...] = acc[rows:]
    for d in range(1, n_tp):
        part_to(d).wait_send()
    for d in range(1, n_ep):
        score_to(d).start()
    score_ref[me] = total[pl.ds(pl.multiple_of(me * 8, 8), 8)]
    for d in range(1, n_ep):
        score_from(d).wait_recv()
    for d in range(1, n_ep):
        score_to(d).wait_send()


def small_sums(scores, norms, n_ep, n_tp):
    cap = scores.shape[1]
    width = norms.shape[1]
    padded = jnp.pad(scores, ((0, 0), (0, 1024 - cap))).reshape(n_ep * 8, 128)
    part = jnp.concatenate([padded, norms.reshape(2 * width // 128, 128)], axis=0)
    norm_out, score_out = pl.pallas_call(
        functools.partial(sums_kernel, n_ep, n_tp),
        out_shape=(
            jax.ShapeDtypeStruct((2 * width // 128, 128), jnp.float32),
            jax.ShapeDtypeStruct((n_ep, 8, 128), jnp.float32),
        ),
        in_specs=[pl.BlockSpec(memory_space=pltpu.VMEM)],
        out_specs=(
            pl.BlockSpec(memory_space=pltpu.VMEM),
            pl.BlockSpec(memory_space=pltpu.VMEM),
        ),
        scratch_shapes=[
            pltpu.VMEM((n_tp,) + part.shape, jnp.float32),
            pltpu.VMEM(part.shape, jnp.float32),
            pltpu.SemaphoreType.DMA((n_tp,)),
            pltpu.SemaphoreType.DMA((n_tp,)),
            pltpu.SemaphoreType.DMA((n_ep,)),
            pltpu.SemaphoreType.DMA((n_ep,)),
        ],
        compiler_params=pltpu.CompilerParams(collective_id=1, has_side_effects=True),
        cost_estimate=pl.CostEstimate(flops=0, bytes_accessed=20_000_000, transcendentals=0),
        name="small_sums",
    )(part)
    return score_out.reshape(n_ep, 1024)[:, :cap], norm_out.reshape(2, width)


def fused_kernel(
    n_ep, n_tp, cap, tok_ref, cot_ref, gate_ref, up_ref, down_ref, route_hbm, group_hbm, prob_hbm,
    token_out, gate_g, up_g, down_g, gate_norm, up_norm, down_norm, prob_grad, group_grad,
    route_ref, group_ref, prob_ref, src_v, gate_v, up_v, down_v, mine, rows, gate_p, up_p, hid_p, pick_v, pick_t,
    part_out, part_in, part_own, part_sum, returned,
    tok_f, tok_b, a_in, b_out, b_in,
    norm_part, norm_in, norm_z, norm_fin, score_part, score_in, score_z, score_tot, score_ep,
    load_sem, sx, rx, zs, zr, fs, fr, ps, pr, es, er, a_s, a_r, b_s, b_r, c_s, c_r, e_s, e_r, q_s, q_r,
    g_s, g_r, f_s, f_r, ns, nr, nzs, nzr, nfs, nfr, ss, sr, szs, szr, ses, ser,
):
    bf, f32 = jnp.bfloat16, jnp.float32
    me = lax.axis_index("ep")
    t = lax.axis_index("tp")
    core = lax.rem(t, 2)
    z = t // 2
    nz = n_tp // 2
    side = lax.rem(z, 2)
    partner = t + 1 - 2 * core
    across = t + 2 - 4 * side
    middle = jnp.logical_and(z > 0, z < nz - 1)
    end = jnp.logical_or(z == 0, z == nz - 1)
    tok, width = token_out.shape
    ff = gate_v.shape[1]
    half = width // 2
    mid_peer = lax.rem(t + 2 * (3 - 2 * z) + n_tp, n_tp)
    peers = {1: me + 1 - 2 * lax.rem(me, 2), 2: lax.rem(me + 2, n_ep), 3: n_ep - 1 - me}

    def remote(src, dst, send, recv, device):
        return pltpu.make_async_remote_copy(
            src_ref=src, dst_ref=dst, send_sem=send, recv_sem=recv,
            device_id=device, device_id_type=MESH,
        )

    @pl.when(core == 0)
    def _():
        pltpu.make_async_copy(tok_ref, src_v, load_sem.at[0]).start()

    @pl.when(core == 1)
    def _():
        pltpu.make_async_copy(cot_ref, src_v, load_sem.at[0]).start()

    small = [
        pltpu.make_async_copy(a, b, load_sem.at[n + 4])
        for n, (a, b) in enumerate(
            ((route_hbm, route_ref), (group_hbm, group_ref), (prob_hbm, prob_ref))
        )
    ]
    for copy in small:
        copy.start()
    loads = [
        pltpu.make_async_copy(a, b, load_sem.at[n + 1])
        for n, (a, b) in enumerate(((gate_ref, gate_v), (up_ref, up_v), (down_ref, down_v)))
    ]
    for copy in loads:
        copy.start()

    barrier = pltpu.get_barrier_semaphore()
    for d in range(1, n_ep):
        pl.semaphore_signal(barrier, inc=1, device_id={"ep": peers[d]}, device_id_type=MESH)
    for d in range(1, nz):
        pl.semaphore_signal(
            barrier, inc=1, device_id={"tp": lax.rem(t + 2 * d, n_tp)}, device_id_type=MESH
        )
    pl.semaphore_signal(barrier, inc=1, device_id={"tp": partner}, device_id_type=MESH)

    for copy in small:
        copy.wait()
    order = [3, 1, 2, 0]
    sends = {3: ((3, 0), (3, 1)), 1: ((1, 0), (1, 1)), 2: ((2, 0), (2, 1), (3, 2), (1, 2), (2, 2))}
    first, second = route_ref[0:1, :], route_ref[1:2, :]
    weight = group_ref[...] * prob_ref[...]
    w0, w1 = weight[0:1, :], weight[1:2, :]
    experts = [me if d == 0 else peers[d] for d in range(n_ep)]
    hit0 = [first == e for e in experts]
    hit1 = [second == e for e in experts]
    named = [jnp.where(jnp.logical_or(x, y), 1.0, 0.0) for x, y in zip(hit0, hit1)]
    weight_of = [jnp.where(x, w0, 0.0) + jnp.where(y, w1, 0.0) for x, y in zip(hit0, hit1)]
    named8 = jnp.concatenate(named + [jnp.zeros((8 - n_ep, tok), f32)], axis=0)
    earlier = jnp.where(
        lax.broadcasted_iota(jnp.int32, (tok, tok), 0) < lax.broadcasted_iota(jnp.int32, (tok, tok), 1),
        1.0, 0.0,
    ).astype(bf)
    before = jnp.dot(named8.astype(bf), earlier, preferred_element_type=f32)
    place = jnp.where(named8 > 0.5, before, -1.0)
    slot = lax.broadcasted_iota(jnp.int32, (cap, tok), 0).astype(f32)
    is_cot = core.astype(f32)
    with jax.named_scope("w_src"):
        pltpu.make_async_copy(tok_ref, src_v, load_sem.at[0]).wait()

    sizes = [cap // 12, cap // 4, cap // 3]
    starts = [0, cap // 12, cap // 3]

    def span(c, s):
        at = starts[c] + s * (cap - 2 * starts[c] - sizes[c])
        return pl.multiple_of(at, 16), sizes[c]

    def block_rows(d, c, s):
        at, n = span(c, s)
        return pl.ds(pl.multiple_of(d * cap + at, 16), n)

    def to_peer(d, c):
        at, n = span(c, side)
        return remote(
            mine.at[d - 1, pl.ds(at, n)], rows.at[core, block_rows(d, c, side)],
            sx.at[d, c], rx.at[d, c], {"ep": peers[d]},
        )

    def swap(d, c, arriving):
        at = block_rows(d, c, 1 - side if arriving else side)
        ref = rows.at[core, at]
        return remote(ref, ref, zs.at[d, c], zr.at[d, c], {"tp": across})

    def share(d, c, swapped, kind):
        if d == 0:
            at = pl.ds(0, cap)
        else:
            at = block_rows(d, c, 1 - side if swapped else side)
        ref = rows.at[kind, at]
        n = c + 3 * swapped
        return remote(ref, ref, fs.at[d, n], fr.at[d, n], {"tp": partner})

    pieces = [(d, c, s) for d in range(1, n_ep) for c, s in ((0, 0), (1, 0), (2, 0), (0, 1), (1, 1))]

    greeted = False
    for d in order:
        with jax.named_scope("mine"):
            pick = jnp.where(slot == place[d:d + 1, :], 1.0, 0.0)
            pick_v[d] = pick.astype(bf)
            slot_weight = jnp.sum(pick * weight_of[d], axis=1, keepdims=True)
            factor = slot_weight * is_cot + (1.0 - is_cot)
            for n in range(0, width, 512):
                got = jnp.dot(pick_v[d], src_v[:, n:n + 512], preferred_element_type=f32)
                got = (got * factor).astype(bf)
                if d == 0:
                    rows[core, 0:cap, n:n + 512] = got
                else:
                    mine[d - 1, :, n:n + 512] = got
            if not greeted:
                with jax.named_scope("barrier"):
                    pl.semaphore_wait(barrier, n_ep - 1 + nz)
                greeted = True
            if d == 0:
                share(0, 0, 0, core).start()
            else:
                for e, c in sends[d]:
                    to_peer(e, c).start()

    column = jnp.transpose(place)
    lane = lax.broadcasted_iota(jnp.int32, (tok, cap), 1).astype(f32)
    for d in range(n_ep):
        pick_t[d] = jnp.where(lane == column[:, d:d + 1], 1.0, 0.0).astype(bf)

    last = (((1,), (1,)), ((), ()))
    contract = (((0,), (0,)), ((), ()))

    def fold(sq):
        parts = [sq[:, j * 128:(j + 1) * 128] for j in range(sq.shape[1] // 128)]
        return functools.reduce(jnp.add, parts)

    mine_half = pl.multiple_of(core * half, 128)
    other_half = pl.multiple_of((1 - core) * half, 128)

    quarter = half // 2

    def exchange(lo, n, h):
        at = pl.ds(lo * cap, n * cap), pl.ds(h * quarter, quarter)
        return remote(
            part_out.at[at], part_in.at[at], ps.at[2 * lo + h], pr.at[2 * lo + h], {"tp": partner}
        )

    jw = 128
    steps = half // jw
    groups = ((0, 1), (1, 2), (3, 1))

    def back(d, j):
        w = jw if d == 3 else 2 * jw
        at = pl.ds(j * w, w)
        return remote(
            part_sum.at[d - 1, :, at], returned.at[d, :, at], es.at[d, j], er.at[d, j], {"ep": peers[d]}
        )

    replies = {
        (3, 0): [(3, j) for j in range(steps // 2)],
        (3, 1): [(3, j) for j in range(steps // 2, steps - 2)],
        (1, 0): [(1, 0), (2, 0), (3, steps - 2), (1, 1), (2, 1), (3, steps - 1)],
        (1, 1): [(d, q) for q in range(2, steps // 2) for d in (1, 2)],
    }

    def block(lo, count, between=()):
        at = slice(lo * cap, (lo + count) * cap)
        score = None
        for n in range(0, ff, 256):
            with jax.named_scope("fwd"):
                pre_gate = jnp.dot(rows[0, at, :], gate_v[:, n:n + 256], preferred_element_type=f32)
                pre_up = jnp.dot(rows[0, at, :], up_v[:, n:n + 256], preferred_element_type=f32)
                grad = lax.dot_general(rows[1, at, :], down_v[n:n + 256, :], last, preferred_element_type=f32)
                sigma = jax.nn.sigmoid(pre_gate)
                activated = pre_gate * sigma
                derivative = sigma * (1.0 + pre_gate * (1.0 - sigma))
                hidden = (activated * pre_up).astype(bf)
                hid_p[at, n:n + 256] = hidden
                more = fold(hidden.astype(f32) * grad)
                score = more if score is None else score + more
                gate_p[at, n:n + 256] = (grad * pre_up * derivative).astype(bf)
                up_p[at, n:n + 256] = (grad * activated).astype(bf)
        for i in range(count):
            score_part[lo + i:lo + i + 1, 0:cap] = jnp.sum(
                jnp.transpose(score[i * cap:(i + 1) * cap]), axis=0, keepdims=True
            )

        def part(c):
            got = lax.dot_general(gate_p[at, :], gate_v[pl.ds(c, 256), :], last, preferred_element_type=f32)
            return got + lax.dot_general(
                up_p[at, :], up_v[pl.ds(c, 256), :], last, preferred_element_type=f32
            )

        for step in between:
            with jax.named_scope("between"):
                step()
        for h in (0, 1):
            with jax.named_scope("part_other"):
                for n in range(h * quarter, (h + 1) * quarter, 256):
                    part_out[at, n:n + 256] = part(pl.multiple_of(other_half + n, 128)).astype(bf)
            exchange(lo, count, h).start()
        for h in (0, 1):
            with jax.named_scope("part_own"):
                for n in range(h * quarter, (h + 1) * quarter, 256):
                    part_own[0:count * cap, n:n + 256] = part(pl.multiple_of(mine_half + n, 128))
            with jax.named_scope("w_part"):
                exchange(lo, count, h).wait_recv()
            for n in range(h * quarter, (h + 1) * quarter, 256):
                total = part_own[0:count * cap, n:n + 256] + part_in[at, n:n + 256].astype(f32)
                total = total.astype(bf)
                for i in range(count):
                    piece = total[i * cap:(i + 1) * cap]
                    if lo == 0:
                        returned[0, :, n:n + 256] = piece
                    else:
                        part_sum[lo + i - 1, :, n:n + 256] = piece
            for d, n in replies.get((lo, h), ()):
                back(d, n).start()

    def arrive(d, c):
        to_peer(d, c).wait_recv()
        if c < 2:
            swap(d, c, False).start()
        share(d, c, 0, core).start()

    def arrive_swap(d, c):
        swap(d, c, True).wait_recv()
        share(d, c, 1, core).start()

    def shared(d):
        for c, s in ((0, 0), (1, 0), (2, 0), (0, 1), (1, 1)):
            share(d, c, s, 1 - core).wait_recv()

    score_part[...] = jnp.zeros_like(score_part)
    with jax.named_scope("w_own"):
        share(0, 0, 0, 1 - core).wait_recv()
        for copy in loads:
            copy.wait()
    block(0, 1, (lambda: arrive(3, 0),))
    with jax.named_scope("w_1"):
        arrive(3, 1)
    with jax.named_scope("w_2"):
        arrive(1, 0)
        arrive(2, 0)
    with jax.named_scope("w_swap0"):
        arrive_swap(3, 0)
        arrive(1, 1)
        arrive(2, 1)
    with jax.named_scope("w_swap1"):
        arrive_swap(3, 1)
        arrive_swap(1, 0)
        arrive_swap(2, 0)
    with jax.named_scope("w_g2"):
        arrive(3, 2)
    with jax.named_scope("w_gsh"):
        shared(3)
    block(3, 1, (lambda: arrive_swap(1, 1),))
    with jax.named_scope("w_xy2"):
        arrive(1, 2)
        arrive(2, 2)
    with jax.named_scope("w_xyswap"):
        arrive_swap(2, 1)
    with jax.named_scope("w_sh12"):
        shared(1)
        shared(2)
    block(1, 2)

    def score_pair():
        return remote(score_part, score_in, ss, sr, {"tp": partner})

    def score_to(d):
        return remote(score_tot, score_z.at[z], szs.at[d], szr.at[d], {"tp": lax.rem(t + 2 * d, n_tp)})

    def score_from(d):
        src = lax.rem(z - d + nz, nz)
        return remote(
            score_tot, score_z.at[src], szs.at[d], szr.at[d], {"tp": lax.rem(t - 2 * d + n_tp, n_tp)}
        )

    def score_back(d):
        return remote(score_fin, score_ep.at[d], ses.at[d], ser.at[d], {"ep": peers[d]})

    score_fin = score_in
    score_pair().start()

    def gate_up(k):
        at = pl.ds(pl.multiple_of(k * 256, 256), 256)
        lhs = rows[0, :, at]
        for n, (rhs, out) in enumerate(((gate_p, gate_g), (up_p, up_g))):
            total = lax.dot_general(lhs, rhs[...], contract, preferred_element_type=f32)
            out[at, :] = total.astype(bf)
            sq = fold(total * total)
            for h in range(2):
                norm_part[n, pl.ds(k * 2 + h, 1), :] = jnp.sum(
                    jnp.transpose(sq[h * 128:(h + 1) * 128]), axis=0, keepdims=True
                ) / (ff * n_tp)

    def loop_gate_up(lo, hi):
        def body(k, carry):
            gate_up(k)
            return carry
        lax.fori_loop(lo, hi, body, 0)

    def down(k):
        at = pl.ds(pl.multiple_of(k * 256, 256), 256)
        lhs = hid_p[:, at]
        sq = None
        for c in range(0, width, 512):
            total = lax.dot_general(lhs, rows[1, :, c:c + 512], contract, preferred_element_type=f32)
            down_g[at, c:c + 512] = total.astype(bf)
            more = fold(total * total)
            sq = more if sq is None else sq + more
        for h in range(2):
            down_norm[0:1, k * 256 + h * 128:k * 256 + (h + 1) * 128] = jnp.sum(
                jnp.transpose(sq[h * 128:(h + 1) * 128]), axis=0, keepdims=True
            ) / width

    def norm_pair():
        return remote(norm_part.at[1 - core], norm_in, ns, nr, {"tp": partner})

    def norm_to(d):
        return remote(norm_part.at[core], norm_z.at[z], nzs.at[d], nzr.at[d],
                      {"tp": lax.rem(t + 2 * d, n_tp)})

    def norm_from(d):
        src = lax.rem(z - d + nz, nz)
        return remote(norm_part.at[core], norm_z.at[src], nzs.at[d], nzr.at[d],
                      {"tp": lax.rem(t - 2 * d + n_tp, n_tp)})

    def norm_done(kind):
        ref = norm_fin.at[kind]
        return remote(ref, ref, nfs, nfr, {"tp": partner})

    def work_score_a():
        score_pair().wait_recv()
        score_pair().wait_send()
        score_tot[...] = score_part[...] + score_in[...]
        for d in range(1, nz):
            score_to(d).start()
        score_z[z] = score_tot[...]

    def work_norm_a():
        norm_pair().start()

    def work_norm_b():
        norm_pair().wait_recv()
        norm_pair().wait_send()
        norm_part[core] = norm_part[core] + norm_in[...]
        for d in range(1, nz):
            norm_to(d).start()
        norm_z[z] = norm_part[core]

    def work_score_b():
        for d in range(1, nz):
            score_from(d).wait_recv()
        score_fin[...] = functools.reduce(jnp.add, [score_z[i] for i in range(nz)])
        for d in range(1, n_ep):
            score_back(d).start()

    def work_norm_c():
        for d in range(1, nz):
            norm_from(d).wait_recv()
        norm_fin[core] = functools.reduce(jnp.add, [norm_z[i] for i in range(nz)])
        norm_done(core).start()

    def work_score_c():
        of0 = jnp.zeros((1, tok), f32)
        of1 = jnp.zeros((1, tok), f32)
        for d in range(n_ep):
            if d:
                score_back(d).wait_recv()
            line = score_fin if d == 0 else score_ep.at[d]
            value = line[d:d + 1, 0:cap]
            top = value.astype(bf).astype(f32)
            rest = value - top
            mid = rest.astype(bf).astype(f32)
            parts = jnp.concatenate([top, mid, rest - mid, jnp.zeros((5, cap), f32)], axis=0)
            hit = jnp.dot(parts.astype(bf), pick_v[d], preferred_element_type=f32)
            hit = hit[0:1, :] + hit[1:2, :] + hit[2:3, :]
            of0 = of0 + jnp.where(hit0[d], hit, 0.0)
            of1 = of1 + jnp.where(hit1[d], hit, 0.0)
        slot0, slot1 = of0 / w0, of1 / w1
        prob_grad[0:1, :] = group_ref[...] * slot0
        prob_grad[1:2, :] = group_ref[...] * slot1
        group_grad[...] = prob_ref[0:1, :] * slot0 + prob_ref[1:2, :] * slot1

    def work_norm_d():
        norm_done(1 - core).wait_recv()
        for i in range(width // 128):
            gate_norm[0:1, i * 128:(i + 1) * 128] = norm_fin[0, i:i + 1, :]
            up_norm[0:1, i * 128:(i + 1) * 128] = norm_fin[1, i:i + 1, :]

    strips = width // 256
    with jax.named_scope("gate_up"):
        loop_gate_up(0, strips // 2)
    with jax.named_scope("score_a"):
        work_score_a()

    th = tok // 2
    own_at = pl.multiple_of((z - 1) * th, 128)
    far_at = pl.multiple_of((2 - z) * th, 128)

    def cols(c, j):
        return pl.ds(pl.multiple_of(c * half + j * jw, 128), jw)

    far_end = lax.rem(t + n_tp // 2, n_tp)
    direct, far = 1, 3
    near_at = pl.multiple_of(jnp.where(z == 0, 0, th), 128)
    beyond_at = pl.multiple_of(jnp.where(z == 0, th, 0), 128)

    def near_copy(j):
        return remote(tok_b.at[j, pl.ds(near_at, th)], a_in.at[j, pl.ds(0, th)], a_s.at[j], a_r.at[j],
                      {"tp": across})

    def beyond_copy(j):
        return remote(tok_b.at[j, pl.ds(beyond_at, th)], a_in.at[j, pl.ds(th, th)], g_s.at[j], g_r.at[j],
                      {"tp": far_end})

    def a_copy(j):
        return remote(tok_b.at[j], a_in.at[j], a_s.at[j], a_r.at[j], {"tp": across})

    def b_copy(j):
        return remote(b_out.at[j], b_in.at[j], b_s.at[j], b_r.at[j], {"tp": mid_peer})

    def c_copy(j, at):
        ref = token_out.at[pl.ds(at, th), cols(core, j)]
        return remote(ref, ref, c_s.at[j], c_r.at[j], {"tp": mid_peer})

    def e_copy(j, at):
        ref = token_out.at[pl.ds(at, th), cols(core, j)]
        return remote(ref, ref, e_s.at[j], e_r.at[j], {"tp": across})

    def q_copy(j, at):
        ref = token_out.at[pl.ds(at, th), cols(core, j)]
        return remote(ref, ref, q_s.at[j], q_r.at[j], {"tp": across})

    def f_copy(j, c):
        ref = token_out.at[:, cols(c, j)]
        return remote(ref, ref, f_s.at[j], f_r.at[j], {"tp": partner})


    def far_copy(j, at):
        ref = token_out.at[pl.ds(at, th), cols(core, j)]
        return remote(ref, ref, q_s.at[j], q_r.at[j], {"tp": far_end})

    lag_a, lag_b, lag_c, lag_e = 1, 3, 5, steps

    def combine(j):
        if j % 2 == 0:
            back(1, j // 2).wait_recv()
            back(2, j // 2).wait_recv()
        back(3, j).wait_recv()
        at = slice(j * jw, (j + 1) * jw)
        total = None
        for d in range(n_ep):
            more = jnp.dot(pick_t[d], returned[d, :, at], preferred_element_type=f32)
            total = more if total is None else total + more

        @pl.when(end)
        def _():
            tok_b[j] = total.astype(bf)
            if j < steps - direct:
                a_copy(j).start()
            else:
                near_copy(j).start()
                beyond_copy(j).start()

        @pl.when(middle)
        def _():
            tok_f[j] = total
            if j >= steps - direct:
                b_out[j] = tok_f[j, pl.ds(far_at, th), :].astype(bf)
                b_copy(j).start()

    def pair_sum(j):
        if j >= steps - direct:
            return

        @pl.when(middle)
        def _():
            a_copy(j).wait_recv()
            b_out[j] = (
                tok_f[j, pl.ds(far_at, th), :] + a_in[j, pl.ds(far_at, th), :].astype(f32)
            ).astype(bf)
            b_copy(j).start()
            tok_f[j, pl.ds(own_at, th), :] = (
                tok_f[j, pl.ds(own_at, th), :] + a_in[j, pl.ds(own_at, th), :].astype(f32)
            )

    def line_sum(j):
        @pl.when(middle)
        def _():
            total = tok_f[j, pl.ds(own_at, th), :]
            if j >= steps - direct:
                near_copy(j).wait_recv()
                beyond_copy(j).wait_recv()
                total = total + a_in[j, 0:th, :].astype(f32) + a_in[j, th:tok, :].astype(f32)
            b_copy(j).wait_recv()
            token_out[pl.ds(own_at, th), cols(core, j)] = (total + b_in[j].astype(f32)).astype(bf)
            c_copy(j, own_at).start()
            e_copy(j, own_at).start()
            if j >= steps - far:
                far_copy(j, own_at).start()

    def relay(j):
        @pl.when(middle)
        def _():
            c_copy(j, far_at).wait_recv()
            if j < steps - far:
                q_copy(j, far_at).start()
            f_copy(j, core).start()

    def collect(j):
        @pl.when(end)
        def _():
            e_copy(j, near_at).wait_recv()
            q_copy(j, beyond_at).wait_recv()
            f_copy(j, core).start()

    filler = {
        1: [lambda: loop_gate_up(strips // 2, strips - 1), work_score_b],
        2: [lambda: loop_gate_up(strips - 1, strips), work_norm_a],
        3: [lambda: down(0)],
        4: [work_norm_b],
        5: [lambda: down(1)],
        steps + 1: [work_score_c],
        steps + 2: [work_norm_c],
    }
    stages = (
        ("combine", 0, combine), ("pair_sum", lag_a, pair_sum), ("line_sum", lag_b, line_sum),
        ("relay", lag_c, relay), ("collect", lag_e, collect),
    )
    for s in range(steps + lag_e):
        for name, lag, step in stages:
            if 0 <= s - lag < steps:
                with jax.named_scope(name):
                    step(s - lag)
            if lag == 0:
                for item in filler.get(s, []):
                    with jax.named_scope("filler"):
                        item()

    with jax.named_scope("last"):
        work_norm_d()

    with jax.named_scope("w_final"):
        for j in range(steps):
            f_copy(j, 1 - core).wait_recv()
            f_copy(j, core).wait_send()
            back(3, j).wait_send()

    @pl.when(end)
    def _():
        for j in range(steps):
            if j < steps - direct:
                a_copy(j).wait_send()
            else:
                near_copy(j).wait_send()
                beyond_copy(j).wait_send()

    @pl.when(middle)
    def _():
        for j in range(steps):
            b_copy(j).wait_send()
            c_copy(j, own_at).wait_send()
            e_copy(j, own_at).wait_send()
            if j < steps - far:
                q_copy(j, far_at).wait_send()
            else:
                far_copy(j, own_at).wait_send()

    for lo, n in groups:
        exchange(lo, n, 0).wait_send()
        exchange(lo, n, 1).wait_send()
    for q in range(steps // 2):
        back(1, q).wait_send()
        back(2, q).wait_send()
    share(0, 0, 0, core).wait_send()
    for d, c, s in pieces:
        share(d, c, s, core).wait_send()
        if not s:
            to_peer(d, c).wait_send()
            if c < 2:
                swap(d, c, False).wait_send()
    for d in range(1, nz):
        score_to(d).wait_send()
        norm_to(d).wait_send()
    for d in range(1, n_ep):
        score_back(d).wait_send()
    norm_done(core).wait_send()


def store_kernel(count, *refs):
    sem = refs[-1]
    copies = [pltpu.make_async_copy(refs[n], refs[count + n], sem.at[n]) for n in range(count)]
    for copy in copies:
        copy.start()
    for copy in copies:
        copy.wait()


def fused(tokens, cotangent, group_prob, expert_prob, routing, gate_weight, up_weight, down_weight):
    tok, width = tokens.shape
    n_ep = lax.axis_size("ep")
    n_tp = lax.axis_size("tp")
    ff = gate_weight.shape[2]
    cap = 3 * tok * routing.shape[1] // (2 * n_ep)
    slots = n_ep * cap
    nz = n_tp // 2
    half = width // 2
    jw = 128
    steps = half // jw
    th = tok // 2
    bf, f32 = jnp.bfloat16, jnp.float32
    vm = pltpu.VMEM
    dma = pltpu.SemaphoreType.DMA
    vmem = pl.BlockSpec(memory_space=pltpu.VMEM)
    hbm = pl.BlockSpec(memory_space=pl.ANY)
    shapes = (
        jax.ShapeDtypeStruct((tok, width), bf),
        jax.ShapeDtypeStruct((width, ff), bf),
        jax.ShapeDtypeStruct((width, ff), bf),
        jax.ShapeDtypeStruct((ff, width), bf),
        jax.ShapeDtypeStruct((1, width), f32),
        jax.ShapeDtypeStruct((1, width), f32),
        jax.ShapeDtypeStruct((1, ff), f32),
        jax.ShapeDtypeStruct((2, tok), f32),
        jax.ShapeDtypeStruct((1, tok), f32),
    )
    count = len(shapes)
    outs = pl.pallas_call(
        functools.partial(fused_kernel, n_ep, n_tp, cap),
        out_shape=tuple(pltpu.VMEM(x.shape, x.dtype) for x in shapes),
        in_specs=[hbm] * 8,
        out_specs=(vmem,) * count,
        scratch_shapes=[
            vm((2, tok), jnp.int32), vm((1, tok), f32), vm((2, tok), f32),
            vm((tok, width), bf), vm((width, ff), bf), vm((width, ff), bf), vm((ff, width), bf),
            vm((n_ep - 1, cap, width), bf), vm((2, slots, width), bf),
            vm((slots, ff), bf), vm((slots, ff), bf), vm((slots, ff), bf),
            vm((n_ep, cap, tok), bf), vm((n_ep, tok, cap), bf),
            vm((slots, half), bf), vm((slots, half), bf), vm((2 * cap, half), f32),
            vm((n_ep - 1, cap, half), bf), vm((n_ep, cap, half), bf),
            vm((steps, tok, jw), f32), vm((steps, tok, jw), bf), vm((steps, tok, jw), bf),
            vm((steps, th, jw), bf), vm((steps, th, jw), bf),
            vm((2, width // 128, 128), f32), vm((width // 128, 128), f32),
            vm((nz, width // 128, 128), f32), vm((2, width // 128, 128), f32),
            vm((8, tok), f32), vm((8, tok), f32), vm((nz, 8, tok), f32), vm((8, tok), f32),
            vm((n_ep, 8, tok), f32),
            dma((7,)), dma((n_ep, 3)), dma((n_ep, 3)), dma((n_ep, 2)), dma((n_ep, 2)),
            dma((n_ep, 5)), dma((n_ep, 5)), dma((2 * n_ep,)), dma((2 * n_ep,)),
            dma((n_ep, steps)), dma((n_ep, steps)),
        ] + [dma((steps,))] * 14 + [
            dma, dma, dma((nz,)), dma((nz,)), dma, dma, dma, dma, dma((nz,)), dma((nz,)),
            dma((n_ep,)), dma((n_ep,)),
        ],
        compiler_params=pltpu.CompilerParams(
            collective_id=3, has_side_effects=True, vmem_limit_bytes=56 << 20
        ),
        name="fused",
    )(
        tokens, cotangent, gate_weight[0], up_weight[0], down_weight[0],
        routing.T, group_prob.reshape(1, tok), expert_prob.T,
    )
    outs = pl.pallas_call(
        functools.partial(store_kernel, count),
        out_shape=shapes,
        in_specs=[vmem] * count,
        out_specs=(hbm,) * count,
        scratch_shapes=[dma((count,))],
        compiler_params=pltpu.CompilerParams(vmem_limit_bytes=1 << 20),
        name="store",
    )(*outs)
    token_grad, gate_g, up_g, down_g, gate_n, up_n, down_n, prob_g, group_g = outs
    return (
        token_grad, group_g.reshape(tok), prob_g.T, gate_g[None], up_g[None], down_g[None],
        gate_n, up_n, down_n,
    )


def general(tokens, cotangent, group_prob, expert_prob, routing, gate_weight, up_weight, down_weight):
    tok_count, model_width = tokens.shape
    top_count = routing.shape[1]
    n_ep = lax.axis_size("ep")
    n_tp = lax.axis_size("tp")
    capacity = 3 * tok_count * top_count // (2 * n_ep)
    buffer_rows = n_ep * capacity
    core = lax.rem(lax.axis_index("tp"), 2)
    weight = group_prob[:, None] * expert_prob

    experts = jnp.arange(n_ep, dtype=jnp.int32)[:, None]
    picks = [routing[None, :, k] == experts for k in range(top_count)]
    named = functools.reduce(jnp.logical_or, picks)
    weight_of = sum(jnp.where(picks[k], weight[None, :, k], 0.0) for k in range(top_count))
    earlier = (
        lax.broadcasted_iota(jnp.int32, (tok_count, tok_count), 0)
        < lax.broadcasted_iota(jnp.int32, (tok_count, tok_count), 1)
    ).astype(jnp.bfloat16)
    before = jnp.dot(named.astype(jnp.bfloat16), earlier, preferred_element_type=jnp.float32)
    place = jnp.where(named, before.astype(jnp.int32), -1)
    filled = place[:, None, :] == lax.broadcasted_iota(jnp.int32, (n_ep, capacity, tok_count), 1)
    pick = filled.astype(jnp.bfloat16).reshape(buffer_rows, tok_count)
    slot_weight = jnp.sum(jnp.where(filled, weight_of[:, None, :], 0.0), axis=2).reshape(buffer_rows, 1)

    source = jnp.where(core == 0, tokens, cotangent)
    factor = jnp.where(core == 0, 1.0, slot_weight)
    mine = jnp.dot(pick, source, preferred_element_type=jnp.float32) * factor
    mine = mine.astype(jnp.bfloat16).reshape(n_ep, capacity, model_width)
    both = dispatch(mine, n_ep)
    flat_in = both[0].reshape(buffer_rows, model_width)
    flat_scaled = both[1].reshape(buffer_rows, model_width)

    w_gate = gate_weight[0]
    w_up = up_weight[0]
    w_down = down_weight[0]
    hidden_total = gate_weight.shape[2] * n_tp
    contract_last = (((1,), (1,)), ((), ()))
    contract_rows = (((0,), (0,)), ((), ()))
    pre_gate = jnp.dot(flat_in, w_gate, preferred_element_type=jnp.float32)
    pre_up = jnp.dot(flat_in, w_up, preferred_element_type=jnp.float32)
    sigma = jax.nn.sigmoid(pre_gate)
    activated = pre_gate * sigma
    derivative = sigma * (1.0 + pre_gate * (1.0 - sigma))
    hidden = (activated * pre_up).astype(jnp.bfloat16)
    hidden_grad = lax.dot_general(
        flat_scaled, w_down, contract_last, preferred_element_type=jnp.float32
    )
    score_part = jnp.sum(hidden.astype(jnp.float32) * hidden_grad, axis=1).reshape(n_ep, capacity)
    gate_pre = (hidden_grad * pre_up * derivative).astype(jnp.bfloat16)
    up_pre = (hidden_grad * activated).astype(jnp.bfloat16)
    input_part = lax.dot_general(
        gate_pre, w_gate, contract_last, preferred_element_type=jnp.float32
    )
    input_part = input_part + lax.dot_general(
        up_pre, w_up, contract_last, preferred_element_type=jnp.float32
    )
    input_part = input_part.astype(jnp.bfloat16).reshape(n_ep, capacity, model_width)
    share = lax.psum_scatter(input_part, "tp", scatter_dimension=2, tiled=True)

    down_sum = lax.dot_general(
        hidden, flat_scaled, contract_rows, preferred_element_type=jnp.float32
    )
    gate_sum = lax.dot_general(flat_in, gate_pre, contract_rows, preferred_element_type=jnp.float32)
    up_sum = lax.dot_general(flat_in, up_pre, contract_rows, preferred_element_type=jnp.float32)
    norm_part = (
        jnp.stack([jnp.sum(gate_sum * gate_sum, axis=1), jnp.sum(up_sum * up_sum, axis=1)])
        / hidden_total
    )
    down_norms = jnp.sum(down_sum * down_sum, axis=1) / model_width
    scores, row_norms = small_sums(score_part, norm_part, n_ep, n_tp)

    share, scores, row_norms, down_norms = lax.optimization_barrier(
        (share, scores, row_norms, down_norms)
    )
    returned = lax.all_to_all(share, "ep", split_axis=0, concat_axis=0, tiled=True)
    returned = returned.reshape(buffer_rows, -1)
    token_share = lax.dot_general(pick, returned, contract_rows, preferred_element_type=jnp.float32)
    token_grad = lax.all_gather(token_share.astype(jnp.bfloat16), "tp", axis=1, tiled=True)
    gate_grad, up_grad, down_grad = (
        x.astype(jnp.bfloat16) for x in (gate_sum, up_sum, down_sum)
    )


    score_of = jnp.sum(jnp.where(filled, scores[:, :, None], 0.0), axis=1)
    slot_score = jnp.stack(
        [jnp.sum(jnp.where(p, score_of, 0.0), axis=0) for p in picks], axis=1
    ) / weight
    expert_prob_grad = group_prob[:, None] * slot_score
    group_prob_grad = jnp.sum(expert_prob * slot_score, axis=1)
    return (
        token_grad,
        group_prob_grad,
        expert_prob_grad,
        gate_grad[None],
        up_grad[None],
        down_grad[None],
        row_norms[0][None],
        row_norms[1][None],
        down_norms[None],
    )


def local(*args):
    n_ep, n_tp = lax.axis_size("ep"), lax.axis_size("tp")
    tok, width = args[0].shape
    ff = args[5].shape[2]
    cap = 3 * tok * args[4].shape[1] // (2 * n_ep)
    fits = cap % 96 == 0 and tok % 256 == 0 and width % 2048 == 0 and ff % 256 == 0
    if n_ep == 4 and n_tp == 8 and args[4].shape[1] == 2 and fits:
        return fused(*args)
    return general(*args)


def solution(mesh):
    return jax.shard_map(
        local,
        mesh=mesh,
        in_specs=(
            P("ep", None),
            P("ep", None),
            P("ep"),
            P("ep", None),
            P("ep", None),
            P("ep", None, "tp"),
            P("ep", None, "tp"),
            P("ep", "tp", None),
        ),
        out_specs=(
            P("ep", None),
            P("ep"),
            P("ep", None),
            P("ep", None, "tp"),
            P("ep", None, "tp"),
            P("ep", "tp", None),
            P("ep", None),
            P("ep", None),
            P("ep", "tp"),
        ),
        check_vma=False,
    )
```

```python
import functools
import jax
import jax.numpy as jnp
from jax import lax
from jax.experimental import pallas as pl
from jax.experimental.pallas import tpu as pltpu
from jax.sharding import PartitionSpec as P

MESH = pl.DeviceIdType.MESH
CHUNKS = 8
DIRECT = 5


def dispatch_kernel(n_ep, mine_ref, out_ref, local_sem, send_sem, recv_sem, fwd_send, fwd_recv, z_send, z_recv):
    me = lax.axis_index("ep")
    t = lax.axis_index("tp")
    core = lax.rem(t, 2)
    partner = t + 1 - 2 * core
    side_z = lax.rem(t // 2, 2)
    across = t + 2 - 4 * side_z
    width = mine_ref.shape[2] // CHUNKS
    barrier = pltpu.get_barrier_semaphore()
    for d in range(1, n_ep):
        pl.semaphore_signal(
            barrier, inc=1, device_id={"ep": lax.rem(me + d, n_ep)}, device_id_type=MESH
        )
    pl.semaphore_signal(barrier, inc=1, device_id={"tp": partner}, device_id_type=MESH)
    pl.semaphore_signal(barrier, inc=1, device_id={"tp": across}, device_id_type=MESH)
    pl.semaphore_wait(barrier, n_ep + 1)

    def cols(c):
        j, side = (c, side_z) if c < DIRECT else (c - DIRECT, 1 - side_z)
        at = j + side * (CHUNKS - 1 - 2 * j)
        return pl.ds(pl.multiple_of(at * width, 128), width)

    def to_peer(d, c):
        dst = lax.rem(me + d, n_ep)
        return pltpu.make_async_remote_copy(
            src_ref=mine_ref.at[dst, :, cols(c)],
            dst_ref=out_ref.at[core, me, :, cols(c)],
            send_sem=send_sem.at[d, c],
            recv_sem=recv_sem.at[d, c],
            device_id={"ep": dst},
            device_id_type=MESH,
        )

    def from_peer(d, c):
        src = lax.rem(me - d + n_ep, n_ep)
        return pltpu.make_async_remote_copy(
            src_ref=mine_ref.at[me, :, cols(c)],
            dst_ref=out_ref.at[core, src, :, cols(c)],
            send_sem=send_sem.at[d, c],
            recv_sem=recv_sem.at[d, c],
            device_id={"ep": src},
            device_id_type=MESH,
        )

    def forward(d, c, side):
        src = lax.rem(me - d + n_ep, n_ep)
        source = mine_ref.at[me, :, cols(c)] if d == 0 else out_ref.at[side, src, :, cols(c)]
        return pltpu.make_async_remote_copy(
            src_ref=source,
            dst_ref=out_ref.at[side, src, :, cols(c)],
            send_sem=fwd_send.at[d, c],
            recv_sem=fwd_recv.at[d, c],
            device_id={"tp": partner},
            device_id_type=MESH,
        )

    def swap(d, c, arriving):
        src = lax.rem(me - d + n_ep, n_ep)
        ref = out_ref.at[core, src, :, cols(c + DIRECT if arriving else c)]
        return pltpu.make_async_remote_copy(
            src_ref=ref,
            dst_ref=ref,
            send_sem=z_send.at[d, c],
            recv_sem=z_recv.at[d, c],
            device_id={"tp": across},
            device_id_type=MESH,
        )

    order = sorted(range(1, n_ep), key=lambda d: abs(d - n_ep // 2))
    extra = CHUNKS - DIRECT
    for c in range(DIRECT):
        for d in order:
            to_peer(d, c).start()
    keep = pltpu.make_async_copy(mine_ref.at[me], out_ref.at[core, me], local_sem)
    keep.start()
    for c in range(CHUNKS):
        forward(0, c, core).start()
    lag = DIRECT - extra
    for c in range(DIRECT):
        for d in order:
            from_peer(d, c).wait_recv()
            if c < extra:
                swap(d, c, False).start()
            forward(d, c, core).start()
        if c >= lag:
            for d in order:
                swap(d, c - lag, True).wait_recv()
                forward(d, c - lag + DIRECT, core).start()
    keep.wait()
    for c in range(DIRECT):
        for d in order:
            to_peer(d, c).wait_send()
    for c in range(extra):
        for d in order:
            swap(d, c, False).wait_send()
    for d in range(n_ep):
        for c in range(CHUNKS):
            forward(d, c, core).wait_send()
            forward(d, c, 1 - core).wait_recv()


def dispatch(mine, n_ep):
    return pl.pallas_call(
        functools.partial(dispatch_kernel, n_ep),
        out_shape=jax.ShapeDtypeStruct((2,) + mine.shape, mine.dtype),
        in_specs=[pl.BlockSpec(memory_space=pltpu.VMEM)],
        out_specs=pl.BlockSpec(memory_space=pl.ANY),
        scratch_shapes=[
            pltpu.SemaphoreType.DMA,
            pltpu.SemaphoreType.DMA((n_ep, CHUNKS)),
            pltpu.SemaphoreType.DMA((n_ep, CHUNKS)),
            pltpu.SemaphoreType.DMA((n_ep, CHUNKS)),
            pltpu.SemaphoreType.DMA((n_ep, CHUNKS)),
            pltpu.SemaphoreType.DMA((n_ep, CHUNKS)),
            pltpu.SemaphoreType.DMA((n_ep, CHUNKS)),
        ],
        compiler_params=pltpu.CompilerParams(collective_id=0, has_side_effects=True),
        name="dispatch",
    )(mine)


def sums_kernel(n_ep, n_tp, part_ref, norm_ref, score_ref, slots, total, send_sem, recv_sem, s_send, s_recv):
    me = lax.axis_index("ep")
    t = lax.axis_index("tp")
    barrier = pltpu.get_barrier_semaphore()
    for d in range(1, n_tp):
        pl.semaphore_signal(
            barrier, inc=1, device_id={"tp": lax.rem(t + d, n_tp)}, device_id_type=MESH
        )
    for d in range(1, n_ep):
        pl.semaphore_signal(
            barrier, inc=1, device_id={"ep": lax.rem(me + d, n_ep)}, device_id_type=MESH
        )
    pl.semaphore_wait(barrier, n_tp - 1 + n_ep - 1)

    def part_to(d):
        return pltpu.make_async_remote_copy(
            src_ref=part_ref,
            dst_ref=slots.at[t],
            send_sem=send_sem.at[d],
            recv_sem=recv_sem.at[d],
            device_id={"tp": lax.rem(t + d, n_tp)},
            device_id_type=MESH,
        )

    def part_from(d):
        src = lax.rem(t - d + n_tp, n_tp)
        return pltpu.make_async_remote_copy(
            src_ref=part_ref,
            dst_ref=slots.at[src],
            send_sem=send_sem.at[d],
            recv_sem=recv_sem.at[d],
            device_id={"tp": src},
            device_id_type=MESH,
        )

    for d in range(1, n_tp):
        part_to(d).start()
    slots[t] = part_ref[...]
    for d in range(1, n_tp):
        part_from(d).wait_recv()
    acc = slots[0]
    for i in range(1, n_tp):
        acc = acc + slots[i]
    total[...] = acc
    rows = 8 * n_ep

    def score_to(d):
        dst = lax.rem(me + d, n_ep)
        return pltpu.make_async_remote_copy(
            src_ref=total.at[pl.ds(pl.multiple_of(dst * 8, 8), 8)],
            dst_ref=score_ref.at[me],
            send_sem=s_send.at[d],
            recv_sem=s_recv.at[d],
            device_id={"ep": dst},
            device_id_type=MESH,
        )

    def score_from(d):
        src = lax.rem(me - d + n_ep, n_ep)
        return pltpu.make_async_remote_copy(
            src_ref=total.at[pl.ds(0, 8)],
            dst_ref=score_ref.at[src],
            send_sem=s_send.at[d],
            recv_sem=s_recv.at[d],
            device_id={"ep": src},
            device_id_type=MESH,
        )

    norm_ref[...] = acc[rows:]
    for d in range(1, n_tp):
        part_to(d).wait_send()
    for d in range(1, n_ep):
        score_to(d).start()
    score_ref[me] = total[pl.ds(pl.multiple_of(me * 8, 8), 8)]
    for d in range(1, n_ep):
        score_from(d).wait_recv()
    for d in range(1, n_ep):
        score_to(d).wait_send()


def small_sums(scores, norms, n_ep, n_tp):
    cap = scores.shape[1]
    width = norms.shape[1]
    padded = jnp.pad(scores, ((0, 0), (0, 1024 - cap))).reshape(n_ep * 8, 128)
    part = jnp.concatenate([padded, norms.reshape(2 * width // 128, 128)], axis=0)
    norm_out, score_out = pl.pallas_call(
        functools.partial(sums_kernel, n_ep, n_tp),
        out_shape=(
            jax.ShapeDtypeStruct((2 * width // 128, 128), jnp.float32),
            jax.ShapeDtypeStruct((n_ep, 8, 128), jnp.float32),
        ),
        in_specs=[pl.BlockSpec(memory_space=pltpu.VMEM)],
        out_specs=(
            pl.BlockSpec(memory_space=pltpu.VMEM),
            pl.BlockSpec(memory_space=pltpu.VMEM),
        ),
        scratch_shapes=[
            pltpu.VMEM((n_tp,) + part.shape, jnp.float32),
            pltpu.VMEM(part.shape, jnp.float32),
            pltpu.SemaphoreType.DMA((n_tp,)),
            pltpu.SemaphoreType.DMA((n_tp,)),
            pltpu.SemaphoreType.DMA((n_ep,)),
            pltpu.SemaphoreType.DMA((n_ep,)),
        ],
        compiler_params=pltpu.CompilerParams(collective_id=1, has_side_effects=True),
        cost_estimate=pl.CostEstimate(flops=0, bytes_accessed=20_000_000, transcendentals=0),
        name="small_sums",
    )(part)
    return score_out.reshape(n_ep, 1024)[:, :cap], norm_out.reshape(2, width)


def fused_kernel(
    n_ep, n_tp, cap, tok_ref, cot_ref, gate_ref, up_ref, down_ref, route_hbm, group_hbm, prob_hbm,
    token_out, gate_g, up_g, down_g, gate_norm, up_norm, down_norm, prob_grad, group_grad,
    route_ref, group_ref, prob_ref, src_v, gate_v, up_v, down_v, mine, rows, gate_p, up_p, hid_p, pick_v, pick_t,
    part_out, part_in, part_own, part_sum, returned,
    early_in, tok_f, tok_b, a_in, b_out, b_in,
    norm_part, norm_in, norm_z, norm_fin, score_part, score_in, score_z, score_tot, score_ep,
    load_sem, sx, rx, zs, zr, fs, fr, ps, pr, es, er, a_s, a_r, b_s, b_r, c_s, c_r, e_s, e_r, q_s, q_r,
    f_s, f_r, p_s, p_r, ns, nr, nzs, nzr, nfs, nfr, ss, sr, szs, szr, ses, ser,
):
    bf, f32 = jnp.bfloat16, jnp.float32
    me = lax.axis_index("ep")
    t = lax.axis_index("tp")
    core = lax.rem(t, 2)
    z = t // 2
    nz = n_tp // 2
    side = lax.rem(z, 2)
    partner = t + 1 - 2 * core
    across = t + 2 - 4 * side
    middle = jnp.logical_and(z > 0, z < nz - 1)
    end = jnp.logical_or(z == 0, z == nz - 1)
    tok, width = token_out.shape
    ff = gate_v.shape[1]
    half = width // 2
    mid_peer = lax.rem(t + 2 * (3 - 2 * z) + n_tp, n_tp)
    peers = {1: me + 1 - 2 * lax.rem(me, 2), 2: lax.rem(me + 2, n_ep), 3: n_ep - 1 - me}

    def remote(src, dst, send, recv, device):
        return pltpu.make_async_remote_copy(
            src_ref=src, dst_ref=dst, send_sem=send, recv_sem=recv,
            device_id=device, device_id_type=MESH,
        )

    @pl.when(core == 0)
    def _():
        pltpu.make_async_copy(tok_ref, src_v, load_sem.at[0]).start()

    @pl.when(core == 1)
    def _():
        pltpu.make_async_copy(cot_ref, src_v, load_sem.at[0]).start()

    small = [
        pltpu.make_async_copy(a, b, load_sem.at[n + 4])
        for n, (a, b) in enumerate(
            ((route_hbm, route_ref), (group_hbm, group_ref), (prob_hbm, prob_ref))
        )
    ]
    for copy in small:
        copy.start()
    loads = [
        pltpu.make_async_copy(a, b, load_sem.at[n + 1])
        for n, (a, b) in enumerate(((gate_ref, gate_v), (up_ref, up_v), (down_ref, down_v)))
    ]
    for copy in loads:
        copy.start()

    barrier = pltpu.get_barrier_semaphore()
    for d in range(1, n_ep):
        pl.semaphore_signal(barrier, inc=1, device_id={"ep": peers[d]}, device_id_type=MESH)
    for d in range(1, nz):
        pl.semaphore_signal(
            barrier, inc=1, device_id={"tp": lax.rem(t + 2 * d, n_tp)}, device_id_type=MESH
        )
    pl.semaphore_signal(barrier, inc=1, device_id={"tp": partner}, device_id_type=MESH)

    for copy in small:
        copy.wait()
    order = [3, 1, 2, 0]
    sends = {3: ((3, 0), (3, 1)), 1: ((1, 0), (1, 1)), 2: ((2, 0), (2, 1), (3, 2), (1, 2), (2, 2))}
    first, second = route_ref[0:1, :], route_ref[1:2, :]
    weight = group_ref[...] * prob_ref[...]
    w0, w1 = weight[0:1, :], weight[1:2, :]
    experts = [me if d == 0 else peers[d] for d in range(n_ep)]
    hit0 = [first == e for e in experts]
    hit1 = [second == e for e in experts]
    named = [jnp.where(jnp.logical_or(x, y), 1.0, 0.0) for x, y in zip(hit0, hit1)]
    weight_of = [jnp.where(x, w0, 0.0) + jnp.where(y, w1, 0.0) for x, y in zip(hit0, hit1)]
    named8 = jnp.concatenate(named + [jnp.zeros((8 - n_ep, tok), f32)], axis=0)
    earlier = jnp.where(
        lax.broadcasted_iota(jnp.int32, (tok, tok), 0) < lax.broadcasted_iota(jnp.int32, (tok, tok), 1),
        1.0, 0.0,
    ).astype(bf)
    before = jnp.dot(named8.astype(bf), earlier, preferred_element_type=f32)
    place = jnp.where(named8 > 0.5, before, -1.0)
    slot = lax.broadcasted_iota(jnp.int32, (cap, tok), 0).astype(f32)
    is_cot = core.astype(f32)
    with jax.named_scope("w_src"):
        pltpu.make_async_copy(tok_ref, src_v, load_sem.at[0]).wait()

    sizes = [cap // 12, cap // 4, cap // 3]
    starts = [0, cap // 12, cap // 3]

    def span(c, s):
        at = starts[c] + s * (cap - 2 * starts[c] - sizes[c])
        return pl.multiple_of(at, 16), sizes[c]

    def block_rows(d, c, s):
        at, n = span(c, s)
        return pl.ds(pl.multiple_of(d * cap + at, 16), n)

    def to_peer(d, c):
        at, n = span(c, side)
        return remote(
            mine.at[d - 1, pl.ds(at, n)], rows.at[core, block_rows(d, c, side)],
            sx.at[d, c], rx.at[d, c], {"ep": peers[d]},
        )

    def swap(d, c, arriving):
        at = block_rows(d, c, 1 - side if arriving else side)
        ref = rows.at[core, at]
        return remote(ref, ref, zs.at[d, c], zr.at[d, c], {"tp": across})

    def share(d, c, swapped, kind):
        if d == 0:
            at = pl.ds(0, cap)
        else:
            at = block_rows(d, c, 1 - side if swapped else side)
        ref = rows.at[kind, at]
        n = c + 3 * swapped
        return remote(ref, ref, fs.at[d, n], fr.at[d, n], {"tp": partner})

    pieces = [(d, c, s) for d in range(1, n_ep) for c, s in ((0, 0), (1, 0), (2, 0), (0, 1), (1, 1))]

    greeted = False
    for d in order:
        with jax.named_scope("mine"):
            pick = jnp.where(slot == place[d:d + 1, :], 1.0, 0.0)
            pick_v[d] = pick.astype(bf)
            slot_weight = jnp.sum(pick * weight_of[d], axis=1, keepdims=True)
            factor = slot_weight * is_cot + (1.0 - is_cot)
            for n in range(0, width, 512):
                got = jnp.dot(pick_v[d], src_v[:, n:n + 512], preferred_element_type=f32)
                got = (got * factor).astype(bf)
                if d == 0:
                    rows[core, 0:cap, n:n + 512] = got
                else:
                    mine[d - 1, :, n:n + 512] = got
            if not greeted:
                with jax.named_scope("barrier"):
                    pl.semaphore_wait(barrier, n_ep - 1 + nz)
                greeted = True
            if d == 0:
                share(0, 0, 0, core).start()
            else:
                for e, c in sends[d]:
                    to_peer(e, c).start()

    column = jnp.transpose(place)
    lane = lax.broadcasted_iota(jnp.int32, (tok, cap), 1).astype(f32)
    for d in range(n_ep):
        pick_t[d] = jnp.where(lane == column[:, d:d + 1], 1.0, 0.0).astype(bf)

    last = (((1,), (1,)), ((), ()))
    contract = (((0,), (0,)), ((), ()))

    def fold(sq):
        parts = [sq[:, j * 128:(j + 1) * 128] for j in range(sq.shape[1] // 128)]
        return functools.reduce(jnp.add, parts)

    mine_half = pl.multiple_of(core * half, 128)
    other_half = pl.multiple_of((1 - core) * half, 128)

    quarter = half // 2

    def exchange(lo, n, h):
        at = pl.ds(lo * cap, n * cap), pl.ds(h * quarter, quarter)
        return remote(
            part_out.at[at], part_in.at[at], ps.at[2 * lo + h], pr.at[2 * lo + h], {"tp": partner}
        )

    jw = 128
    steps = half // jw
    groups = ((0, 1), (1, 2), (3, 1))
    piece_at = (0, 1, 4, 5, 6, 7, 2, 3)
    early = 2
    early_q = piece_at[-1] // 2
    early_cols = slice(early_q * 2 * jw, (early_q + 1) * 2 * jw)

    def early_copy(d):
        src = returned.at[0, :, early_cols] if d == 0 else part_sum.at[d - 1, :, early_cols]
        return remote(src, early_in.at[d], p_s.at[d], p_r.at[d], {"tp": across})

    def early_sum(ds):
        @pl.when(middle)
        def _():
            for d in ds:
                early_copy(d).wait_recv()
                own = returned[0, :, early_cols] if d == 0 else part_sum[d - 1, :, early_cols]
                total = (own.astype(f32) + early_in[d].astype(f32)).astype(bf)
                if d == 0:
                    returned[0, :, early_cols] = total
                else:
                    part_sum[d - 1, :, early_cols] = total
                for n in (steps - 2, steps - 1) if d == 3 else (early_q,) if d else ():
                    back(d, n).start()

    def back(d, j):
        at = pl.ds(piece_at[j] * jw, jw) if d == 3 else pl.ds(j * 2 * jw, 2 * jw)
        return remote(
            part_sum.at[d - 1, :, at], returned.at[d, :, at], es.at[d, j], er.at[d, j], {"ep": peers[d]}
        )

    replies = {
        (3, 0): [(3, 0), (3, 1)],
        (3, 1): [(3, 2), (3, 3)],
        (1, 0): [(1, 0), (2, 0), (3, 4)],
        (1, 1): [(1, 2), (2, 2), (3, 5), (1, 3), (2, 3)],
    }

    def block(lo, count, between=()):
        at = slice(lo * cap, (lo + count) * cap)
        score = None
        for n in range(0, ff, 256):
            with jax.named_scope("fwd"):
                pre_gate = jnp.dot(rows[0, at, :], gate_v[:, n:n + 256], preferred_element_type=f32)
                pre_up = jnp.dot(rows[0, at, :], up_v[:, n:n + 256], preferred_element_type=f32)
                grad = lax.dot_general(rows[1, at, :], down_v[n:n + 256, :], last, preferred_element_type=f32)
                sigma = jax.nn.sigmoid(pre_gate)
                activated = pre_gate * sigma
                derivative = sigma * (1.0 + pre_gate * (1.0 - sigma))
                hidden = (activated * pre_up).astype(bf)
                hid_p[at, n:n + 256] = hidden
                more = fold(hidden.astype(f32) * grad)
                score = more if score is None else score + more
                gate_p[at, n:n + 256] = (grad * pre_up * derivative).astype(bf)
                up_p[at, n:n + 256] = (grad * activated).astype(bf)
        for i in range(count):
            score_part[lo + i:lo + i + 1, 0:cap] = jnp.sum(
                jnp.transpose(score[i * cap:(i + 1) * cap]), axis=0, keepdims=True
            )

        def part(c):
            got = lax.dot_general(gate_p[at, :], gate_v[pl.ds(c, 256), :], last, preferred_element_type=f32)
            return got + lax.dot_general(
                up_p[at, :], up_v[pl.ds(c, 256), :], last, preferred_element_type=f32
            )

        for step in between:
            with jax.named_scope("between"):
                step()
        for h in (0, 1):
            with jax.named_scope("part_other"):
                for n in range(h * quarter, (h + 1) * quarter, 256):
                    part_out[at, n:n + 256] = part(pl.multiple_of(other_half + n, 128)).astype(bf)
            exchange(lo, count, h).start()
        for h in (0, 1):
            with jax.named_scope("part_own"):
                for n in range(h * quarter, (h + 1) * quarter, 256):
                    part_own[0:count * cap, n:n + 256] = part(pl.multiple_of(mine_half + n, 128))
            with jax.named_scope("w_part"):
                exchange(lo, count, h).wait_recv()
            for n in range(h * quarter, (h + 1) * quarter, 256):
                total = part_own[0:count * cap, n:n + 256] + part_in[at, n:n + 256].astype(f32)
                total = total.astype(bf)
                for i in range(count):
                    piece = total[i * cap:(i + 1) * cap]
                    if lo == 0:
                        returned[0, :, n:n + 256] = piece
                    else:
                        part_sum[lo + i - 1, :, n:n + 256] = piece
            for d, n in replies.get((lo, h), ()):
                back(d, n).start()
            if h == early_q // 2:
                @pl.when(end)
                def _():
                    for d in range(lo, lo + count):
                        early_copy(d).start()

    def arrive(d, c):
        to_peer(d, c).wait_recv()
        if c < 2:
            swap(d, c, False).start()
        share(d, c, 0, core).start()

    def arrive_swap(d, c):
        swap(d, c, True).wait_recv()
        share(d, c, 1, core).start()

    def shared(d):
        for c, s in ((0, 0), (1, 0), (2, 0), (0, 1), (1, 1)):
            share(d, c, s, 1 - core).wait_recv()

    score_part[...] = jnp.zeros_like(score_part)
    with jax.named_scope("w_own"):
        share(0, 0, 0, 1 - core).wait_recv()
        for copy in loads:
            copy.wait()
    block(0, 1, (lambda: arrive(3, 0),))
    with jax.named_scope("w_1"):
        arrive(3, 1)
    with jax.named_scope("w_2"):
        arrive(1, 0)
        arrive(2, 0)
    with jax.named_scope("w_swap0"):
        arrive_swap(3, 0)
        arrive(1, 1)
        arrive(2, 1)
    with jax.named_scope("w_swap1"):
        arrive_swap(3, 1)
        arrive_swap(1, 0)
        arrive_swap(2, 0)
    with jax.named_scope("w_g2"):
        arrive(3, 2)
    with jax.named_scope("w_gsh"):
        shared(3)
    block(3, 1, (lambda: arrive_swap(1, 1),))
    with jax.named_scope("w_xy2"):
        arrive(1, 2)
        arrive(2, 2)
    with jax.named_scope("w_xyswap"):
        arrive_swap(2, 1)
    with jax.named_scope("w_sh12"):
        shared(1)
        shared(2)
    block(1, 2, (lambda: early_sum((0, 3)),))

    def score_pair():
        return remote(score_part, score_in, ss, sr, {"tp": partner})

    def score_to(d):
        return remote(score_tot, score_z.at[z], szs.at[d], szr.at[d], {"tp": lax.rem(t + 2 * d, n_tp)})

    def score_from(d):
        src = lax.rem(z - d + nz, nz)
        return remote(
            score_tot, score_z.at[src], szs.at[d], szr.at[d], {"tp": lax.rem(t - 2 * d + n_tp, n_tp)}
        )

    def score_back(d):
        return remote(score_fin, score_ep.at[d], ses.at[d], ser.at[d], {"ep": peers[d]})

    score_fin = score_in
    score_pair().start()

    def gate_up(k):
        at = pl.ds(pl.multiple_of(k * 256, 256), 256)
        lhs = rows[0, :, at]
        for n, (rhs, out) in enumerate(((gate_p, gate_g), (up_p, up_g))):
            total = lax.dot_general(lhs, rhs[...], contract, preferred_element_type=f32)
            out[at, :] = total.astype(bf)
            sq = fold(total * total)
            for h in range(2):
                norm_part[n, pl.ds(k * 2 + h, 1), :] = jnp.sum(
                    jnp.transpose(sq[h * 128:(h + 1) * 128]), axis=0, keepdims=True
                ) / (ff * n_tp)

    def loop_gate_up(lo, hi):
        def body(k, carry):
            gate_up(k)
            return carry
        lax.fori_loop(lo, hi, body, 0)

    def down(k):
        at = pl.ds(pl.multiple_of(k * 256, 256), 256)
        lhs = hid_p[:, at]
        sq = None
        for c in range(0, width, 512):
            total = lax.dot_general(lhs, rows[1, :, c:c + 512], contract, preferred_element_type=f32)
            down_g[at, c:c + 512] = total.astype(bf)
            more = fold(total * total)
            sq = more if sq is None else sq + more
        for h in range(2):
            down_norm[0:1, k * 256 + h * 128:k * 256 + (h + 1) * 128] = jnp.sum(
                jnp.transpose(sq[h * 128:(h + 1) * 128]), axis=0, keepdims=True
            ) / width

    def norm_pair():
        return remote(norm_part.at[1 - core], norm_in, ns, nr, {"tp": partner})

    def norm_to(d):
        return remote(norm_part.at[core], norm_z.at[z], nzs.at[d], nzr.at[d],
                      {"tp": lax.rem(t + 2 * d, n_tp)})

    def norm_from(d):
        src = lax.rem(z - d + nz, nz)
        return remote(norm_part.at[core], norm_z.at[src], nzs.at[d], nzr.at[d],
                      {"tp": lax.rem(t - 2 * d + n_tp, n_tp)})

    def norm_done(kind):
        ref = norm_fin.at[kind]
        return remote(ref, ref, nfs, nfr, {"tp": partner})

    def work_score_a():
        score_pair().wait_recv()
        score_pair().wait_send()
        score_tot[...] = score_part[...] + score_in[...]
        for d in range(1, nz):
            score_to(d).start()
        score_z[z] = score_tot[...]

    def work_norm_a():
        norm_pair().start()

    def work_norm_b():
        norm_pair().wait_recv()
        norm_pair().wait_send()
        norm_part[core] = norm_part[core] + norm_in[...]
        for d in range(1, nz):
            norm_to(d).start()
        norm_z[z] = norm_part[core]

    def work_score_b():
        for d in range(1, nz):
            score_from(d).wait_recv()
        score_fin[...] = functools.reduce(jnp.add, [score_z[i] for i in range(nz)])
        for d in range(1, n_ep):
            score_back(d).start()

    def work_norm_c():
        for d in range(1, nz):
            norm_from(d).wait_recv()
        norm_fin[core] = functools.reduce(jnp.add, [norm_z[i] for i in range(nz)])
        norm_done(core).start()

    def work_score_c():
        of0 = jnp.zeros((1, tok), f32)
        of1 = jnp.zeros((1, tok), f32)
        for d in range(n_ep):
            if d:
                score_back(d).wait_recv()
            line = score_fin if d == 0 else score_ep.at[d]
            value = line[d:d + 1, 0:cap]
            top = value.astype(bf).astype(f32)
            rest = value - top
            mid = rest.astype(bf).astype(f32)
            parts = jnp.concatenate([top, mid, rest - mid, jnp.zeros((5, cap), f32)], axis=0)
            hit = jnp.dot(parts.astype(bf), pick_v[d], preferred_element_type=f32)
            hit = hit[0:1, :] + hit[1:2, :] + hit[2:3, :]
            of0 = of0 + jnp.where(hit0[d], hit, 0.0)
            of1 = of1 + jnp.where(hit1[d], hit, 0.0)
        slot0, slot1 = of0 / w0, of1 / w1
        prob_grad[0:1, :] = group_ref[...] * slot0
        prob_grad[1:2, :] = group_ref[...] * slot1
        group_grad[...] = prob_ref[0:1, :] * slot0 + prob_ref[1:2, :] * slot1

    def work_norm_d():
        norm_done(1 - core).wait_recv()
        for i in range(width // 128):
            gate_norm[0:1, i * 128:(i + 1) * 128] = norm_fin[0, i:i + 1, :]
            up_norm[0:1, i * 128:(i + 1) * 128] = norm_fin[1, i:i + 1, :]

    strips = width // 256
    with jax.named_scope("gate_up"):
        loop_gate_up(0, strips // 2)
    with jax.named_scope("score_a"):
        work_score_a()

    th = tok // 2
    own_at = pl.multiple_of((z - 1) * th, 128)
    far_at = pl.multiple_of((2 - z) * th, 128)

    def cols(c, j):
        return pl.ds(pl.multiple_of(c * half + piece_at[j] * jw, 128), jw)

    far_end = lax.rem(t + n_tp // 2, n_tp)
    far = 3
    near_at = pl.multiple_of(jnp.where(z == 0, 0, th), 128)
    beyond_at = pl.multiple_of(jnp.where(z == 0, th, 0), 128)

    def a_copy(j):
        return remote(tok_b.at[j], a_in.at[j], a_s.at[j], a_r.at[j], {"tp": across})

    def b_copy(j):
        return remote(b_out.at[j], b_in.at[j], b_s.at[j], b_r.at[j], {"tp": mid_peer})

    def c_copy(j, at):
        ref = token_out.at[pl.ds(at, th), cols(core, j)]
        return remote(ref, ref, c_s.at[j], c_r.at[j], {"tp": mid_peer})

    def e_copy(j, at):
        ref = token_out.at[pl.ds(at, th), cols(core, j)]
        return remote(ref, ref, e_s.at[j], e_r.at[j], {"tp": across})

    def q_copy(j, at):
        ref = token_out.at[pl.ds(at, th), cols(core, j)]
        return remote(ref, ref, q_s.at[j], q_r.at[j], {"tp": across})

    def f_copy(j, c):
        ref = token_out.at[:, cols(c, j)]
        return remote(ref, ref, f_s.at[j], f_r.at[j], {"tp": partner})


    def far_copy(j, at):
        ref = token_out.at[pl.ds(at, th), cols(core, j)]
        return remote(ref, ref, q_s.at[j], q_r.at[j], {"tp": far_end})

    lag_a, lag_b, lag_c, lag_e = 1, 3, 5, steps

    def combine(j):
        if j >= steps - early:
            @pl.when(middle)
            def _():
                total = token_part(j)
                tok_f[j] = total
                b_out[j] = tok_f[j, pl.ds(far_at, th), :].astype(bf)
                b_copy(j).start()

            return
        total = token_part(j)

        @pl.when(end)
        def _():
            tok_b[j] = total.astype(bf)
            a_copy(j).start()

        @pl.when(middle)
        def _():
            tok_f[j] = total

    def token_part(j):
        if j % 2 == 0:
            back(1, piece_at[j] // 2).wait_recv()
            back(2, piece_at[j] // 2).wait_recv()
        back(3, j).wait_recv()
        at = slice(piece_at[j] * jw, (piece_at[j] + 1) * jw)
        total = None
        for d in range(n_ep):
            more = jnp.dot(pick_t[d], returned[d, :, at], preferred_element_type=f32)
            total = more if total is None else total + more
        return total

    def pair_sum(j):
        if j >= steps - early:
            return

        @pl.when(middle)
        def _():
            a_copy(j).wait_recv()
            b_out[j] = (
                tok_f[j, pl.ds(far_at, th), :] + a_in[j, pl.ds(far_at, th), :].astype(f32)
            ).astype(bf)
            b_copy(j).start()
            tok_f[j, pl.ds(own_at, th), :] = (
                tok_f[j, pl.ds(own_at, th), :] + a_in[j, pl.ds(own_at, th), :].astype(f32)
            )

    def line_sum(j):
        @pl.when(middle)
        def _():
            total = tok_f[j, pl.ds(own_at, th), :]
            b_copy(j).wait_recv()
            token_out[pl.ds(own_at, th), cols(core, j)] = (total + b_in[j].astype(f32)).astype(bf)
            c_copy(j, own_at).start()
            e_copy(j, own_at).start()
            if j >= steps - far:
                far_copy(j, own_at).start()

    def relay(j):
        @pl.when(middle)
        def _():
            c_copy(j, far_at).wait_recv()
            if j < steps - far:
                q_copy(j, far_at).start()
            f_copy(j, core).start()

    def collect(j):
        @pl.when(end)
        def _():
            e_copy(j, near_at).wait_recv()
            q_copy(j, beyond_at).wait_recv()
            f_copy(j, core).start()

    filler = {
        1: [lambda: early_sum((1, 2)), lambda: loop_gate_up(strips // 2, strips - 1), work_score_b],
        2: [lambda: loop_gate_up(strips - 1, strips), work_norm_a],
        3: [lambda: down(0)],
        4: [work_norm_b],
        5: [lambda: down(1)],
        steps + 1: [work_score_c],
        steps + 2: [work_norm_c],
    }
    stages = (
        ("combine", 0, combine), ("pair_sum", lag_a, pair_sum), ("line_sum", lag_b, line_sum),
        ("relay", lag_c, relay), ("collect", lag_e, collect),
    )
    for s in range(steps + lag_e):
        for name, lag, step in stages:
            if 0 <= s - lag < steps:
                with jax.named_scope(name):
                    step(s - lag)
            if lag == 0:
                for item in filler.get(s, []):
                    with jax.named_scope("filler"):
                        item()

    with jax.named_scope("last"):
        work_norm_d()

    with jax.named_scope("w_final"):
        for j in range(steps):
            f_copy(j, 1 - core).wait_recv()
            f_copy(j, core).wait_send()
            if j < steps - early:
                back(3, j).wait_send()

    @pl.when(end)
    def _():
        for j in range(steps):
            if j < steps - early:
                a_copy(j).wait_send()
        for d in range(n_ep):
            early_copy(d).wait_send()

    @pl.when(middle)
    def _():
        for j in range(steps):
            b_copy(j).wait_send()
            c_copy(j, own_at).wait_send()
            e_copy(j, own_at).wait_send()
            if j < steps - far:
                q_copy(j, far_at).wait_send()
            else:
                far_copy(j, own_at).wait_send()

    for lo, n in groups:
        exchange(lo, n, 0).wait_send()
        exchange(lo, n, 1).wait_send()
    for q in range(steps // 2):
        if q != early_q:
            back(1, q).wait_send()
            back(2, q).wait_send()

    @pl.when(middle)
    def _():
        back(1, early_q).wait_send()
        back(2, early_q).wait_send()
        for j in range(steps - early, steps):
            back(3, j).wait_send()

    share(0, 0, 0, core).wait_send()
    for d, c, s in pieces:
        share(d, c, s, core).wait_send()
        if not s:
            to_peer(d, c).wait_send()
            if c < 2:
                swap(d, c, False).wait_send()
    for d in range(1, nz):
        score_to(d).wait_send()
        norm_to(d).wait_send()
    for d in range(1, n_ep):
        score_back(d).wait_send()
    norm_done(core).wait_send()


def store_kernel(count, *refs):
    sem = refs[-1]
    copies = [pltpu.make_async_copy(refs[n], refs[count + n], sem.at[n]) for n in range(count)]
    for copy in copies:
        copy.start()
    for copy in copies:
        copy.wait()


def fused(tokens, cotangent, group_prob, expert_prob, routing, gate_weight, up_weight, down_weight):
    tok, width = tokens.shape
    n_ep = lax.axis_size("ep")
    n_tp = lax.axis_size("tp")
    ff = gate_weight.shape[2]
    cap = 3 * tok * routing.shape[1] // (2 * n_ep)
    slots = n_ep * cap
    nz = n_tp // 2
    half = width // 2
    jw = 128
    steps = half // jw
    th = tok // 2
    bf, f32 = jnp.bfloat16, jnp.float32
    vm = pltpu.VMEM
    dma = pltpu.SemaphoreType.DMA
    vmem = pl.BlockSpec(memory_space=pltpu.VMEM)
    hbm = pl.BlockSpec(memory_space=pl.ANY)
    shapes = (
        jax.ShapeDtypeStruct((tok, width), bf),
        jax.ShapeDtypeStruct((width, ff), bf),
        jax.ShapeDtypeStruct((width, ff), bf),
        jax.ShapeDtypeStruct((ff, width), bf),
        jax.ShapeDtypeStruct((1, width), f32),
        jax.ShapeDtypeStruct((1, width), f32),
        jax.ShapeDtypeStruct((1, ff), f32),
        jax.ShapeDtypeStruct((2, tok), f32),
        jax.ShapeDtypeStruct((1, tok), f32),
    )
    count = len(shapes)
    outs = pl.pallas_call(
        functools.partial(fused_kernel, n_ep, n_tp, cap),
        out_shape=tuple(pltpu.VMEM(x.shape, x.dtype) for x in shapes),
        in_specs=[hbm] * 8,
        out_specs=(vmem,) * count,
        scratch_shapes=[
            vm((2, tok), jnp.int32), vm((1, tok), f32), vm((2, tok), f32),
            vm((tok, width), bf), vm((width, ff), bf), vm((width, ff), bf), vm((ff, width), bf),
            vm((n_ep - 1, cap, width), bf), vm((2, slots, width), bf),
            vm((slots, ff), bf), vm((slots, ff), bf), vm((slots, ff), bf),
            vm((n_ep, cap, tok), bf), vm((n_ep, tok, cap), bf),
            vm((slots, half), bf), vm((slots, half), bf), vm((2 * cap, half), f32),
            vm((n_ep - 1, cap, half), bf), vm((n_ep, cap, half), bf),
            vm((n_ep, cap, 2 * jw), bf),
            vm((steps, tok, jw), f32), vm((steps, tok, jw), bf), vm((steps, tok, jw), bf),
            vm((steps, th, jw), bf), vm((steps, th, jw), bf),
            vm((2, width // 128, 128), f32), vm((width // 128, 128), f32),
            vm((nz, width // 128, 128), f32), vm((2, width // 128, 128), f32),
            vm((8, tok), f32), vm((8, tok), f32), vm((nz, 8, tok), f32), vm((8, tok), f32),
            vm((n_ep, 8, tok), f32),
            dma((7,)), dma((n_ep, 3)), dma((n_ep, 3)), dma((n_ep, 2)), dma((n_ep, 2)),
            dma((n_ep, 5)), dma((n_ep, 5)), dma((2 * n_ep,)), dma((2 * n_ep,)),
            dma((n_ep, steps)), dma((n_ep, steps)),
        ] + [dma((steps,))] * 12 + [dma((n_ep,)), dma((n_ep,))] + [
            dma, dma, dma((nz,)), dma((nz,)), dma, dma, dma, dma, dma((nz,)), dma((nz,)),
            dma((n_ep,)), dma((n_ep,)),
        ],
        compiler_params=pltpu.CompilerParams(
            collective_id=3, has_side_effects=True, vmem_limit_bytes=56 << 20
        ),
        name="fused",
    )(
        tokens, cotangent, gate_weight[0], up_weight[0], down_weight[0],
        routing.T, group_prob.reshape(1, tok), expert_prob.T,
    )
    outs = pl.pallas_call(
        functools.partial(store_kernel, count),
        out_shape=shapes,
        in_specs=[vmem] * count,
        out_specs=(hbm,) * count,
        scratch_shapes=[dma((count,))],
        compiler_params=pltpu.CompilerParams(vmem_limit_bytes=1 << 20),
        name="store",
    )(*outs)
    token_grad, gate_g, up_g, down_g, gate_n, up_n, down_n, prob_g, group_g = outs
    return (
        token_grad, group_g.reshape(tok), prob_g.T, gate_g[None], up_g[None], down_g[None],
        gate_n, up_n, down_n,
    )


def general(tokens, cotangent, group_prob, expert_prob, routing, gate_weight, up_weight, down_weight):
    tok_count, model_width = tokens.shape
    top_count = routing.shape[1]
    n_ep = lax.axis_size("ep")
    n_tp = lax.axis_size("tp")
    capacity = 3 * tok_count * top_count // (2 * n_ep)
    buffer_rows = n_ep * capacity
    core = lax.rem(lax.axis_index("tp"), 2)
    weight = group_prob[:, None] * expert_prob

    experts = jnp.arange(n_ep, dtype=jnp.int32)[:, None]
    picks = [routing[None, :, k] == experts for k in range(top_count)]
    named = functools.reduce(jnp.logical_or, picks)
    weight_of = sum(jnp.where(picks[k], weight[None, :, k], 0.0) for k in range(top_count))
    earlier = (
        lax.broadcasted_iota(jnp.int32, (tok_count, tok_count), 0)
        < lax.broadcasted_iota(jnp.int32, (tok_count, tok_count), 1)
    ).astype(jnp.bfloat16)
    before = jnp.dot(named.astype(jnp.bfloat16), earlier, preferred_element_type=jnp.float32)
    place = jnp.where(named, before.astype(jnp.int32), -1)
    filled = place[:, None, :] == lax.broadcasted_iota(jnp.int32, (n_ep, capacity, tok_count), 1)
    pick = filled.astype(jnp.bfloat16).reshape(buffer_rows, tok_count)
    slot_weight = jnp.sum(jnp.where(filled, weight_of[:, None, :], 0.0), axis=2).reshape(buffer_rows, 1)

    source = jnp.where(core == 0, tokens, cotangent)
    factor = jnp.where(core == 0, 1.0, slot_weight)
    mine = jnp.dot(pick, source, preferred_element_type=jnp.float32) * factor
    mine = mine.astype(jnp.bfloat16).reshape(n_ep, capacity, model_width)
    both = dispatch(mine, n_ep)
    flat_in = both[0].reshape(buffer_rows, model_width)
    flat_scaled = both[1].reshape(buffer_rows, model_width)

    w_gate = gate_weight[0]
    w_up = up_weight[0]
    w_down = down_weight[0]
    hidden_total = gate_weight.shape[2] * n_tp
    contract_last = (((1,), (1,)), ((), ()))
    contract_rows = (((0,), (0,)), ((), ()))
    pre_gate = jnp.dot(flat_in, w_gate, preferred_element_type=jnp.float32)
    pre_up = jnp.dot(flat_in, w_up, preferred_element_type=jnp.float32)
    sigma = jax.nn.sigmoid(pre_gate)
    activated = pre_gate * sigma
    derivative = sigma * (1.0 + pre_gate * (1.0 - sigma))
    hidden = (activated * pre_up).astype(jnp.bfloat16)
    hidden_grad = lax.dot_general(
        flat_scaled, w_down, contract_last, preferred_element_type=jnp.float32
    )
    score_part = jnp.sum(hidden.astype(jnp.float32) * hidden_grad, axis=1).reshape(n_ep, capacity)
    gate_pre = (hidden_grad * pre_up * derivative).astype(jnp.bfloat16)
    up_pre = (hidden_grad * activated).astype(jnp.bfloat16)
    input_part = lax.dot_general(
        gate_pre, w_gate, contract_last, preferred_element_type=jnp.float32
    )
    input_part = input_part + lax.dot_general(
        up_pre, w_up, contract_last, preferred_element_type=jnp.float32
    )
    input_part = input_part.astype(jnp.bfloat16).reshape(n_ep, capacity, model_width)
    share = lax.psum_scatter(input_part, "tp", scatter_dimension=2, tiled=True)

    down_sum = lax.dot_general(
        hidden, flat_scaled, contract_rows, preferred_element_type=jnp.float32
    )
    gate_sum = lax.dot_general(flat_in, gate_pre, contract_rows, preferred_element_type=jnp.float32)
    up_sum = lax.dot_general(flat_in, up_pre, contract_rows, preferred_element_type=jnp.float32)
    norm_part = (
        jnp.stack([jnp.sum(gate_sum * gate_sum, axis=1), jnp.sum(up_sum * up_sum, axis=1)])
        / hidden_total
    )
    down_norms = jnp.sum(down_sum * down_sum, axis=1) / model_width
    scores, row_norms = small_sums(score_part, norm_part, n_ep, n_tp)

    share, scores, row_norms, down_norms = lax.optimization_barrier(
        (share, scores, row_norms, down_norms)
    )
    returned = lax.all_to_all(share, "ep", split_axis=0, concat_axis=0, tiled=True)
    returned = returned.reshape(buffer_rows, -1)
    token_share = lax.dot_general(pick, returned, contract_rows, preferred_element_type=jnp.float32)
    token_grad = lax.all_gather(token_share.astype(jnp.bfloat16), "tp", axis=1, tiled=True)
    gate_grad, up_grad, down_grad = (
        x.astype(jnp.bfloat16) for x in (gate_sum, up_sum, down_sum)
    )


    score_of = jnp.sum(jnp.where(filled, scores[:, :, None], 0.0), axis=1)
    slot_score = jnp.stack(
        [jnp.sum(jnp.where(p, score_of, 0.0), axis=0) for p in picks], axis=1
    ) / weight
    expert_prob_grad = group_prob[:, None] * slot_score
    group_prob_grad = jnp.sum(expert_prob * slot_score, axis=1)
    return (
        token_grad,
        group_prob_grad,
        expert_prob_grad,
        gate_grad[None],
        up_grad[None],
        down_grad[None],
        row_norms[0][None],
        row_norms[1][None],
        down_norms[None],
    )


def local(*args):
    n_ep, n_tp = lax.axis_size("ep"), lax.axis_size("tp")
    tok, width = args[0].shape
    ff = args[5].shape[2]
    cap = 3 * tok * args[4].shape[1] // (2 * n_ep)
    fits = cap % 96 == 0 and tok % 256 == 0 and width % 2048 == 0 and ff % 256 == 0
    if n_ep == 4 and n_tp == 8 and args[4].shape[1] == 2 and fits:
        return fused(*args)
    return general(*args)


def solution(mesh):
    return jax.shard_map(
        local,
        mesh=mesh,
        in_specs=(
            P("ep", None),
            P("ep", None),
            P("ep"),
            P("ep", None),
            P("ep", None),
            P("ep", None, "tp"),
            P("ep", None, "tp"),
            P("ep", "tp", None),
        ),
        out_specs=(
            P("ep", None),
            P("ep"),
            P("ep", None),
            P("ep", None, "tp"),
            P("ep", None, "tp"),
            P("ep", "tp", None),
            P("ep", None),
            P("ep", None),
            P("ep", "tp"),
        ),
        check_vma=False,
    )
```
